32 devices in a mesh: grp: 2 (over x), ep: 4 (over y, core), tp: 4 (over z).
Axes of the slice: x: 2, y: 2, z: 4, core: 2. Of those that a mesh axis runs over, the one named last changes fastest.
Arguments:
- mixer_in: bfloat16 [4096, 2048], P(('grp', 'ep', 'tp')), parts along dimension 0, may hold values from -600 to 600
- mixer_gain: float32 [2048], replicated, may hold values from 0.1 to 1.9
- w_query: bfloat16 [2048, 1024], P(None, 'tp'), may hold values from -6 to 6
- w_key: bfloat16 [2048, 512], P(None, 'tp'), may hold values from -0.1875 to 0.1875
- w_value: bfloat16 [2048, 512], P(None, 'tp'), may hold values from -0.25 to 0.25
- sink_logit: float32 [16], P('tp'), may hold values from 3 to 9
- moe_in: bfloat16 [4096, 2048], P(('grp', 'ep', 'tp')), parts along dimension 0, may hold values from -600 to 600
- moe_gain: float32 [2048], replicated, may hold values from 0.1 to 1.9
- router: bfloat16 [2048, 16], replicated, may hold values from -0.25 to 0.25
- routes: int32 [4096, 4], P(('grp', 'ep', 'tp')), parts along dimension 0, may hold values from 0 to 15, all different within a row; in each aligned block of 128 rows (0 to 127, 128 to 255, ...) at most 48 rows name the same one
- expert_gate: bfloat16 [16, 2048, 512], P(('ep', 'tp')), may hold values from -0.125 to 0.125
- expert_up: bfloat16 [16, 2048, 512], P(('ep', 'tp')), may hold values from -0.125 to 0.125
- expert_down: bfloat16 [16, 512, 2048], P(('ep', 'tp')), may hold values from -0.25 to 0.25
- shared_gate: bfloat16 [2048, 512], P(None, 'tp'), may hold values from -0.125 to 0.125
- shared_up: bfloat16 [2048, 512], P(None, 'tp'), may hold values from -0.125 to 0.125
- shared_down: bfloat16 [512, 2048], P('tp'), may hold values from -0.25 to 0.25
Outputs:
- mixed: bfloat16 [4096, 1024], P(('grp', 'ep'), 'tp'), parts along dimension 0
- moe_out: bfloat16 [4096, 2048], P(('grp', 'ep', 'tp')), parts along dimension 0
The draws below stay inside these ranges and needn't reach their ends.
There are 2 independent parts, one for each index of `grp`. The reference program is written for one: setup_inputs(seed, part) draws one part's arguments, and reference() takes and returns one part's arrays. A program takes and returns all parts, laid end to end along the dimension named above; an argument that names none is the same for every part. Nothing has to cross between parts.
Inputs may be any that keep to these rules, and one draw needn't show every extreme that they name: `routes`: each row names 4 different experts. Within the rows of one device (aligned blocks of 128 rows) no expert is named by more than 48 rows, a bound that some block reaches.
All inputs are finite; a program needn't handle non-finite values.
Results may differ from the reference program's by a relative error of at most 0.012.
Values may be sent and summed in bfloat16 or wider, within the bound.
A program may use at most 128 MiB of HBM per device.

```python
import math
import jax
import jax.numpy as jnp
import numpy as np
from jax import lax

D = 2048
HEADS = 16
KV_HEADS = 8
HEAD_DIM = 64
WINDOW = 128
EFF = 512
SFF = 512
TOP_K = 4
ROWS = 128
TOKENS = 2048
EXPERTS = 16
CAP = 48


def draw_mixer_in(key, part):
    values = jnp.clip(jax.random.normal(jax.random.fold_in(key, 1), (TOKENS, D), jnp.float32), -6.0, 6.0)
    return values.astype(jnp.bfloat16)


def draw_moe_in(key, part):
    values = jnp.clip(jax.random.normal(jax.random.fold_in(key, 4), (TOKENS, D), jnp.float32), -6.0, 6.0)
    return values.astype(jnp.bfloat16)


def attention_weights(key):
    key_part, query_part = jax.random.split(jax.random.fold_in(key, 7), 2)
    spread = (2.0 / D) ** 0.5
    keys_weight = jnp.clip(jax.random.normal(key_part, (D, KV_HEADS, HEAD_DIM), jnp.float32), -6.0, 6.0) * spread
    query_weight = jnp.clip(jax.random.normal(query_part, (D, HEADS, HEAD_DIM), jnp.float32), -6.0, 6.0) * spread
    return (query_weight.reshape(D, HEADS * HEAD_DIM), keys_weight.reshape(D, KV_HEADS * HEAD_DIM))


def draw_w_query(key, part):
    return attention_weights(key)[0].astype(jnp.bfloat16)


def draw_w_key(key, part):
    return attention_weights(key)[1].astype(jnp.bfloat16)


def shard_levels(key, extent, pieces, low, high):
    gain, own = 1.0, jax.random.fold_in(key, 6)
    for axis_at, parts in pieces:
        steps = jnp.exp(jax.random.uniform(jax.random.fold_in(own, axis_at), (parts,), jnp.float32, low / len(pieces), high / len(pieces)))
        gain = gain * jnp.repeat(steps, extent[axis_at] // parts).reshape([-1 if axis == axis_at else 1 for axis in range(len(extent))])
    return gain


def shared_out(stream_key, own, number, rows, amount, top, bound, skew):
    order = jax.random.permutation(stream_key, amount)
    heavy_load, usual = shares(amount, rows * top, bound, skew, True), shares(amount, rows * top, bound, skew, False)
    places = jnp.arange(amount)

    def named(lengths, offset_by):
        used = int((lengths > 0).sum())
        fixed = max(1, used // 4)
        shifted = fixed + (places - fixed + offset_by * (used - fixed)) % max(1, amount - fixed)
        return jnp.zeros((amount,), jnp.int32).at[order[jnp.where(places < fixed, places, shifted)]].set(jnp.asarray(lengths, jnp.int32))

    lengths = jnp.where(number % 4 == 0, named(heavy_load, number // 4), named(usual, number - number // 4 - 1))
    mixed = jax.random.permutation(jax.random.fold_in(own, 3), amount)
    giver, taker = mixed[0:amount // 2 * 2:2], mixed[1:amount // 2 * 2:2]
    margin = jnp.minimum(lengths[giver] - 1, bound - lengths[taker]) // 2
    margin = jnp.where((giver == order[0]) | (taker == order[0]) | (lengths[taker] == 0), 0, jnp.maximum(margin, 0))
    shifted = jax.random.randint(jax.random.fold_in(own, 4), (amount // 2,), 0, 1 << 20) % (margin + 1)
    lengths = lengths.at[giver].add(-shifted).at[taker].add(shifted)
    members = jnp.searchsorted(jnp.cumsum(lengths), jnp.arange(rows * top), side="right").astype(jnp.int32)
    listing = members.reshape(top, rows).T
    listing = listing[jax.random.permutation(jax.random.fold_in(own, 1), rows)]
    offset_by = jax.random.randint(jax.random.fold_in(own, 2), (rows, 1), 0, top)
    return jnp.take_along_axis(listing, (jnp.arange(top)[None, :] + offset_by) % top, axis=1)


def shares(amount, total, bound, skew, full):
    weights = [(1 << 20) // math.isqrt(grade ** skew) + 1 for grade in range(1, amount + 1)]
    largest = bound if full else min(bound, max(-(-total // amount), total * weights[0] // sum(weights)))
    least = 1 if total - largest >= amount - 1 else 0
    given, surplus = [largest] + [least] * (amount - 1), total - largest - least * (amount - 1)
    while surplus > 0:
        movable = [i for i in range(1, amount) if given[i] < largest] or [i for i in range(1, amount) if given[i] < bound]
        pool, remaining = sum([weights[i] for i in movable]), surplus
        for i in movable:
            extra = min(bound - given[i], max(1, remaining * weights[i] // pool), surplus)
            given[i] = given[i] + extra
            surplus = surplus - extra
    return np.array(given)


def bell_draw(key, shape, scale, limit, cuts=(), kind=jnp.bfloat16):
    array = jax.random.normal(key, shape, jnp.float32) * scale
    if len(cuts) > 0:
        array = shard_levels(key, shape, cuts, -0.22, 0.18) * array
    return jnp.clip(array, min=-limit, max=limit).astype(kind)


def setup_inputs(seed: int = 0, part: int = 0) -> dict:
    key_list = jax.random.split(jax.random.key(seed), 17)
    own_keys = jax.random.split(jax.random.fold_in(key_list[16], part), 17)
    mixer_in = draw_mixer_in(jax.random.fold_in(jax.random.fold_in(key_list[16], part), 71), part)
    mixer_gain = jnp.clip(1.0 + 0.18 * jax.random.normal(key_list[1], (D,), jnp.float32), 0.1, 1.9)
    w_query = draw_w_query(jax.random.fold_in(key_list[16], 71), part)
    w_key = draw_w_key(jax.random.fold_in(key_list[16], 71), part)
    w_value = bell_draw(key_list[4], (D, KV_HEADS * HEAD_DIM), (D // 4) ** -0.5, 0.25, ((1, 4),))
    sink_logit = jnp.clip(3.0 + 6.0 * jax.random.uniform(key_list[5], (HEADS,), jnp.float32) ** shard_levels(key_list[5], (HEADS,), ((0, 4),), -0.2, 0.2), 3.0, 9.0)
    moe_in = draw_moe_in(jax.random.fold_in(jax.random.fold_in(key_list[16], part), 71), part)
    moe_gain = jnp.clip(1.0 + 0.18 * jax.random.normal(key_list[7], (D,), jnp.float32), 0.1, 1.9)
    router = bell_draw(key_list[8], (D, EXPERTS), (D // 4) ** -0.5, 0.25)
    routes_keys = jax.random.split(jax.random.fold_in(own_keys[9], 1), TOKENS // ROWS)
    routes_turns = jax.random.permutation(jax.random.fold_in(own_keys[9], 3), TOKENS // ROWS)
    routes = jax.vmap(lambda own, number: shared_out(jax.random.fold_in(own_keys[9], 2), own, number, ROWS, EXPERTS, TOP_K, CAP, 2))(routes_keys, routes_turns).reshape((TOKENS, TOP_K))
    expert_gate = bell_draw(key_list[10], (EXPERTS, D, EFF), D ** -0.5, 0.125, ((0, 16),))
    expert_up = bell_draw(key_list[11], (EXPERTS, D, EFF), D ** -0.5, 0.125, ((0, 16),))
    expert_down = bell_draw(key_list[12], (EXPERTS, EFF, D), EFF ** -0.5, 0.25, ((0, 16),))
    shared_gate = bell_draw(key_list[13], (D, SFF), D ** -0.5, 0.125, ((1, 4),))
    shared_up = bell_draw(key_list[14], (D, SFF), D ** -0.5, 0.125, ((1, 4),))
    shared_down = bell_draw(key_list[15], (SFF, D), SFF ** -0.5, 0.25, ((0, 4),))
    return dict(mixer_in=mixer_in, mixer_gain=mixer_gain, w_query=w_query, w_key=w_key, w_value=w_value, sink_logit=sink_logit, moe_in=moe_in, moe_gain=moe_gain, router=router, routes=routes, expert_gate=expert_gate, expert_up=expert_up, expert_down=expert_down, shared_gate=shared_gate, shared_up=shared_up, shared_down=shared_down)


EPS = 1e-06
THETA = 10000.0
ROUTED_SCALE = 2.5

def rms_rows(row_block, gain_vector):
    values = row_block.astype(jnp.float32)
    factor = lax.rsqrt(lax.optimization_barrier(jnp.mean(values * values, axis=-1, keepdims=True)) + EPS)
    return (values * factor * gain_vector.astype(jnp.float32)).astype(jnp.bfloat16)

def rotate(head_rows, positions):
    half_width = head_rows.shape[-1] // 2
    inverse = THETA ** (-(jnp.arange(half_width, dtype=jnp.float32) * 2.0) / head_rows.shape[-1])
    angles = positions.astype(jnp.float32)[:, None] * inverse[None, :]
    cosine_table = jnp.cos(angles)[:, None, :]
    sine_table = jnp.sin(angles)[:, None, :]
    first_half = head_rows[..., :half_width]
    second_half = head_rows[..., half_width:]
    return jnp.concatenate([first_half * cosine_table - second_half * sine_table, second_half * cosine_table + first_half * sine_table], axis=-1)

def window_attention(query_rows, key_rows, value_rows, sink_logit):
    length = query_rows.shape[0]
    head_count = query_rows.shape[1]
    kv_count = key_rows.shape[1]
    group_size = head_count // kv_count
    head_width = query_rows.shape[2]
    block_rows = min(512, length)
    padding = ((WINDOW, WINDOW), (0, 0), (0, 0))
    key_table = jnp.pad(key_rows, padding)
    value_table = jnp.pad(value_rows, padding)
    grouped = query_rows.reshape(length, kv_count, group_size, head_width)
    row_ids = jnp.arange(block_rows, dtype=jnp.int32)[:, None]
    col_ids = jnp.arange(block_rows + 2 * WINDOW, dtype=jnp.int32)[None, :]
    sink_table = sink_logit.astype(jnp.float32).reshape(kv_count, group_size)[:, :, None, None]

    def one_block(block_index):
        block_start = block_index * block_rows
        query_block = lax.dynamic_slice_in_dim(grouped, block_start, block_rows, 0).astype(jnp.float32)
        key_block = lax.dynamic_slice_in_dim(key_table, block_start, block_rows + 2 * WINDOW, 0).astype(jnp.float32)
        value_block = lax.dynamic_slice_in_dim(value_table, block_start, block_rows + 2 * WINDOW, 0).astype(jnp.float32)
        scores = jnp.einsum('qkgd,ckd->kgqc', query_block, key_block) * head_width ** (-0.5)
        key_pos = block_start - WINDOW + col_ids
        query_pos = block_start + row_ids
        in_window = (jnp.abs(key_pos - query_pos) <= WINDOW) & (key_pos >= 0) & (key_pos < length)
        scores = jnp.where(in_window[None, None], scores, -jnp.inf)
        row_max = jnp.maximum(lax.optimization_barrier(jnp.max(scores, axis=-1, keepdims=True)), sink_table)
        weights = jnp.exp(scores - row_max)
        denominator = lax.optimization_barrier(jnp.sum(weights, axis=-1, keepdims=True)) + jnp.exp(sink_table - row_max)
        probability = (weights / denominator).astype(jnp.bfloat16)
        output = jnp.einsum('kgqc,ckd->qkgd', probability.astype(jnp.float32), value_block)
        return output.reshape(block_rows, head_count * head_width).astype(jnp.bfloat16)
    blocks_out = lax.map(one_block, jnp.arange(length // block_rows, dtype=jnp.int32))
    return blocks_out.reshape(length, head_count * head_width)

def reference(mixer_in, mixer_gain, w_query, w_key, w_value, sink_logit, moe_in, moe_gain, router, routes, expert_gate, expert_up, expert_down, shared_gate, shared_up, shared_down):
    normed_first = rms_rows(mixer_in, mixer_gain)
    positions = jnp.arange(normed_first.shape[0], dtype=jnp.int32)
    query_rows = rotate(jnp.dot(normed_first, w_query, preferred_element_type=jnp.float32).reshape(-1, HEADS, HEAD_DIM), positions).astype(jnp.bfloat16)
    key_rows = rotate(jnp.dot(normed_first, w_key, preferred_element_type=jnp.float32).reshape(-1, KV_HEADS, HEAD_DIM), positions).astype(jnp.bfloat16)
    value_rows = jnp.dot(normed_first, w_value, preferred_element_type=jnp.float32).astype(jnp.bfloat16)
    value_rows = value_rows.reshape(-1, KV_HEADS, HEAD_DIM)
    mixed = window_attention(query_rows, key_rows, value_rows, sink_logit)
    normed_second = rms_rows(moe_in, moe_gain)
    affinity = jax.nn.sigmoid(jnp.dot(normed_second, router, preferred_element_type=jnp.float32))
    chosen = jnp.take_along_axis(affinity, routes, axis=1)
    route_weight = ROUTED_SCALE * chosen / lax.optimization_barrier(jnp.sum(chosen, axis=-1, keepdims=True))
    shared_hidden = (jax.nn.silu(jnp.dot(normed_second, shared_gate, preferred_element_type=jnp.float32)) * jnp.dot(normed_second, shared_up, preferred_element_type=jnp.float32)).astype(jnp.bfloat16)
    shared = jnp.dot(shared_hidden, shared_down, preferred_element_type=jnp.float32)
    token_count = routes.shape[0]
    sources = token_count // ROWS
    per_source = routes.reshape(sources, ROWS * TOP_K)
    one_hot = (per_source[:, :, None] == jnp.arange(EXPERTS, dtype=jnp.int32)[None, None, :]).astype(jnp.int32)
    slot_index = lax.optimization_barrier(jnp.sum((jnp.cumsum(one_hot, axis=1) - 1) * one_hot, axis=-1))
    source_ids = jnp.arange(sources, dtype=jnp.int32)[:, None]
    column = (source_ids * CAP + slot_index).reshape(-1).astype(jnp.int32)
    token_ids = jnp.arange(token_count * TOP_K, dtype=jnp.int32) // TOP_K
    flat_routes = routes.reshape(-1)
    row_table = jnp.full((EXPERTS, sources * CAP), token_count, jnp.int32).at[flat_routes, column].set(token_ids)
    weight_table = jnp.zeros((EXPERTS, sources * CAP), jnp.float32).at[flat_routes, column].set(route_weight.reshape(-1))
    padded_rows = jnp.concatenate([normed_second, jnp.zeros((1, normed_second.shape[1]), jnp.bfloat16)], axis=0)

    def one_expert(totals, inputs):
        row_ids, scales, gate_weight, up_weight, down_weight = inputs
        gathered = padded_rows[row_ids]
        hidden = (jax.nn.silu(jnp.dot(gathered, gate_weight, preferred_element_type=jnp.float32)) * jnp.dot(gathered, up_weight, preferred_element_type=jnp.float32)).astype(jnp.bfloat16)
        result = jnp.dot(hidden, down_weight, preferred_element_type=jnp.float32).astype(jnp.bfloat16)
        return (totals.at[row_ids].add(result.astype(jnp.float32) * scales[:, None]), None)
    totals, _ = lax.scan(one_expert, jnp.zeros((token_count + 1, normed_second.shape[1]), jnp.float32), (row_table, weight_table, expert_gate, expert_up, expert_down))
    moe_out = (totals[:token_count] + shared).astype(jnp.bfloat16)
    return (mixed, moe_out)
```

```python
import functools

import jax
import jax.numpy as jnp
from jax import lax
from jax.experimental import pallas as pl
from jax.experimental.pallas import tpu as pltpu
from jax.sharding import PartitionSpec as P

HEAD_DIM = 64
WINDOW = 128


EPS = 1e-06
THETA = 10000.0
ROUTED_SCALE = 2.5


def extended(block, sides, width):
    for axis, dim in sides:
        count = lax.axis_size(axis)
        forward = [(i, i + 1) for i in range(count - 1)]
        backward = [(target, source) for source, target in forward]
        low = lax.ppermute(
            lax.slice_in_dim(block, block.shape[dim] - width, None, axis=dim), axis, forward
        )
        high = lax.ppermute(lax.slice_in_dim(block, 0, width, axis=dim), axis, backward)
        block = jnp.concatenate([low, block, high], axis=dim)
    return block


def rms_rows(row_block, gain_vector):
    values = row_block.astype(jnp.float32)
    factor = lax.rsqrt(jnp.mean(values * values, axis=-1, keepdims=True) + EPS)
    return (values * factor * gain_vector).astype(jnp.bfloat16)


def rotate(head_rows, positions):
    half_width = head_rows.shape[-1] // 2
    inverse = THETA ** (-(jnp.arange(half_width, dtype=jnp.float32) * 2.0) / head_rows.shape[-1])
    angles = positions.astype(jnp.float32)[:, None] * inverse[None, :]
    cosine_table = jnp.cos(angles)[:, None, :]
    sine_table = jnp.sin(angles)[:, None, :]
    first_half = head_rows[..., :half_width]
    second_half = head_rows[..., half_width:]
    return jnp.concatenate(
        [
            first_half * cosine_table - second_half * sine_table,
            second_half * cosine_table + first_half * sine_table,
        ],
        axis=-1,
    )


def attend(query_rows, stacked, sink_logit, offset, seq_length):
    span_rows, head_count, head_width = query_rows.shape
    kv_local = stacked.shape[1] // (2 * head_width)
    group_size = head_count // kv_local
    key_table = stacked[:, : kv_local * head_width].reshape(-1, kv_local, head_width)
    value_table = stacked[:, kv_local * head_width :].reshape(-1, kv_local, head_width)
    block_rows = 512
    grouped = query_rows.reshape(span_rows, kv_local, group_size, head_width)
    row_ids = jnp.arange(block_rows, dtype=jnp.int32)[:, None]
    col_ids = jnp.arange(block_rows + 2 * WINDOW, dtype=jnp.int32)[None, :]
    sink_table = sink_logit.reshape(kv_local, group_size)[:, :, None, None]

    def one_block(block_index):
        block_start = block_index * block_rows
        query_block = lax.dynamic_slice_in_dim(grouped, block_start, block_rows, 0)
        key_block = lax.dynamic_slice_in_dim(key_table, block_start, block_rows + 2 * WINDOW, 0)
        value_block = lax.dynamic_slice_in_dim(value_table, block_start, block_rows + 2 * WINDOW, 0)
        scores = jnp.einsum(
            "qkgd,ckd->kgqc", query_block, key_block, preferred_element_type=jnp.float32
        ) * head_width ** (-0.5)
        key_pos = offset + block_start - WINDOW + col_ids
        query_pos = offset + block_start + row_ids
        in_window = (
            (jnp.abs(key_pos - query_pos) <= WINDOW) & (key_pos >= 0) & (key_pos < seq_length)
        )
        scores = jnp.where(in_window[None, None], scores, -jnp.inf)
        row_max = jnp.maximum(jnp.max(scores, axis=-1, keepdims=True), sink_table)
        weights = jnp.exp(scores - row_max)
        denominator = jnp.sum(weights, axis=-1, keepdims=True) + jnp.exp(sink_table - row_max)
        probability = (weights / denominator).astype(jnp.bfloat16)
        output = jnp.einsum(
            "kgqc,ckd->qkgd", probability, value_block, preferred_element_type=jnp.float32
        )
        return output.reshape(block_rows, head_count * head_width).astype(jnp.bfloat16)

    blocks_out = lax.map(one_block, jnp.arange(span_rows // block_rows, dtype=jnp.int32))
    return blocks_out.reshape(span_rows, head_count * head_width)


MESH = pl.DeviceIdType.MESH
VMEM_LIMIT = 60 * 2**20
CHUNK = 512


def remote(src, dst, send_sem, recv_sem, device):
    return pltpu.make_async_remote_copy(
        src_ref=src,
        dst_ref=dst,
        send_sem=send_sem,
        recv_sem=recv_sem,
        device_id=device,
        device_id_type=MESH,
    )


def entry_barrier(grp, ep, tp, ep_count, tp_count):
    barrier = pltpu.get_barrier_semaphore()

    @pl.when(tp > 0)
    def _():
        pl.semaphore_signal(barrier, inc=1, device_id=(grp, ep, tp - 1), device_id_type=MESH)

    @pl.when(tp < tp_count - 1)
    def _():
        pl.semaphore_signal(barrier, inc=1, device_id=(grp, ep, tp + 1), device_id_type=MESH)

    for d in range(1, ep_count):
        pl.semaphore_signal(
            barrier, inc=1, device_id=(grp, lax.rem(ep + d, ep_count), tp), device_id_type=MESH
        )

    inner = (tp > 0) & (tp < tp_count - 1)
    pl.semaphore_wait(barrier, ep_count + jnp.where(inner, 1, 0))


def dispatch_kernel(
    ep_count, tp_count, second, first, meta, gath2, gath1, metag, disp, sbuf,
    own_sem, s2, r2, sm, rm, s1, r1, sd, rd, ld,
):
    grp, ep, tp = lax.axis_index("grp"), lax.axis_index("ep"), lax.axis_index("tp")
    rows, width = second.shape
    slots = disp.shape[2]
    entry_barrier(grp, ep, tp, ep_count, tp_count)
    locals_ = [
        pltpu.make_async_copy(second, gath2.at[tp], own_sem.at[0]),
        pltpu.make_async_copy(meta, metag.at[tp], own_sem.at[1]),
        pltpu.make_async_copy(first, gath1.at[tp], own_sem.at[2]),
    ]

    def toward(side):
        return (grp, ep, tp + (1 if side == 0 else -1))

    def exists(side):
        return tp < tp_count - 1 if side == 0 else tp > 0

    def send_second(side, block, own):
        return [
            remote(second if own else gath2.at[block], gath2.at[block], s2.at[side, block], r2.at[block], toward(side)),
            remote(meta if own else metag.at[block], metag.at[block], sm.at[side, block], rm.at[block], toward(side)),
        ]

    def send_first(side, block, own):
        return remote(first if own else gath1.at[block], gath1.at[block], s1.at[side, block], r1.at[block], toward(side))

    def start_own_first(side, step):
        last = tp if side == 0 else tp_count - 1 - tp

        @pl.when(exists(side) & (step == last))
        def _():
            send_first(side, tp, True).start()

    def dispatch_copy(block, d):
        return remote(
            sbuf.at[block, pl.ds(d * slots, slots)], disp.at[ep, block], sd.at[block, d], rd.at[block, d],
            (grp, lax.rem(ep + d, ep_count), tp),
        )

    def local_dispatch(block):
        return pltpu.make_async_copy(sbuf.at[block, pl.ds(0, slots)], disp.at[ep, block], ld.at[block])

    def process(block):
        slot_ids = lax.broadcasted_iota(jnp.int32, (slots, rows), 0).astype(jnp.float32)
        picks = []
        for d in range(ep_count):
            expert = lax.rem(ep + d, ep_count) * tp_count + tp
            places = metag[block, pl.ds(expert, 1), :]
            picks.append(jnp.where(slot_ids == places, 1.0, 0.0))
        pick = jnp.concatenate(picks, axis=0).astype(jnp.bfloat16)

        def columns(c, carry):
            span = pl.ds(pl.multiple_of(c * CHUNK, CHUNK), CHUNK)
            sbuf[block, :, span] = jnp.dot(
                pick, gath2[block, :, span], preferred_element_type=jnp.float32
            ).astype(jnp.bfloat16)
            return carry

        lax.fori_loop(0, width // CHUNK, columns, 0)
        for d in range(1, ep_count):
            dispatch_copy(block, d).start()
        local_dispatch(block).start()

    for side in range(2):

        @pl.when(exists(side))
        def _():
            for copy in send_second(side, tp, True):
                copy.start()

        start_own_first(side, 0)
    for copy in locals_:
        copy.start()
    locals_[0].wait()
    locals_[1].wait()
    process(tp)

    def hop(k, carry):
        for side in range(2):
            block = tp - k if side == 0 else tp + k
            inside = block >= 0 if side == 0 else block < tp_count

            @pl.when(inside)
            def _():
                for copy in send_second(side, block, False):
                    copy.wait_recv()

                @pl.when(exists(side))
                def _():
                    for copy in send_second(side, block, False):
                        copy.start()

            start_own_first(side, k)

            @pl.when(inside)
            def _():
                process(block)

        return carry

    lax.fori_loop(1, tp_count, hop, 0)
    locals_[2].wait()

    def hop_first(k, carry):
        for side in range(2):
            block = tp - k if side == 0 else tp + k
            inside = block >= 0 if side == 0 else block < tp_count

            @pl.when(inside)
            def _():
                send_first(side, block, False).wait_recv()

                @pl.when(exists(side))
                def _():
                    send_first(side, block, False).start()

        return carry

    lax.fori_loop(1, tp_count, hop_first, 0)

    def finish(block, carry):
        for d in range(1, ep_count):
            dispatch_copy(block, d).wait()
        local_dispatch(block).wait()
        for side in range(2):
            passed = block <= tp if side == 0 else block >= tp

            @pl.when(exists(side) & passed)
            def _():
                for copy in send_second(side, block, False):
                    copy.wait_send()
                send_first(side, block, False).wait_send()

        return carry

    lax.fori_loop(0, tp_count, finish, 0)


def dispatch(second, first, meta, ep_count, tp_count, slots):
    rows, width = second.shape
    vmem = pl.BlockSpec(memory_space=pltpu.VMEM)
    dma = pltpu.SemaphoreType.DMA
    return pl.pallas_call(
        functools.partial(dispatch_kernel, ep_count, tp_count),
        out_shape=(
            jax.ShapeDtypeStruct((tp_count, rows, width), jnp.bfloat16),
            jax.ShapeDtypeStruct((tp_count, rows, width), jnp.bfloat16),
            jax.ShapeDtypeStruct((tp_count,) + meta.shape, jnp.float32),
            jax.ShapeDtypeStruct((ep_count, tp_count, slots, width), jnp.bfloat16),
        ),
        in_specs=[vmem] * 3,
        out_specs=(vmem,) * 4,
        scratch_shapes=[
            pltpu.VMEM((tp_count, ep_count * slots, width), jnp.bfloat16),
            dma((3,)),
            dma((2, tp_count)),
            dma((tp_count,)),
            dma((2, tp_count)),
            dma((tp_count,)),
            dma((2, tp_count)),
            dma((tp_count,)),
            dma((tp_count, ep_count)),
            dma((tp_count, ep_count)),
            dma((tp_count,)),
        ],
        compiler_params=pltpu.CompilerParams(
            collective_id=0, has_side_effects=True, vmem_limit_bytes=VMEM_LIMIT
        ),
        name="dispatch",
    )(second, first, meta)


def combine_kernel(
    ep_count, tp_count, results, hidden, down, metag, out, back, rin, lin, psend,
    sb, rb, lb, sp, rr, rl,
):
    grp, ep, tp = lax.axis_index("grp"), lax.axis_index("ep"), lax.axis_index("tp")
    rows, width = out.shape
    slots = results.shape[2]
    experts = metag.shape[1] // 2
    entry_barrier(grp, ep, tp, ep_count, tp_count)

    def return_copy(block, d):
        target = lax.rem(ep + d, ep_count)
        return remote(
            results.at[target, block], back.at[block, pl.ds(d * slots, slots)], sb.at[block, d], rb.at[block, d],
            (grp, target, tp),
        )

    def local_return(block):
        return pltpu.make_async_copy(results.at[ep, block], back.at[block, pl.ds(0, slots)], lb.at[block])

    def start_return(block):
        for d in range(1, ep_count):
            return_copy(block, d).start()
        local_return(block).start()

    def wait_return(block):
        for d in range(1, ep_count):
            return_copy(block, d).wait_recv()
        local_return(block).wait()

    def pass_on(side, block):
        return remote(
            psend.at[block],
            (rin if side == 0 else lin).at[block],
            sp.at[block],
            (rr if side == 0 else rl).at[block],
            (grp, ep, tp + (1 if side == 0 else -1)),
        )

    def begin(k, carry):
        @pl.when(tp_count - 1 - k > tp)
        def _():
            start_return(tp_count - 1 - k)

        @pl.when(k < tp)
        def _():
            start_return(k)

        return carry

    lax.fori_loop(0, tp_count - 1, begin, 0)
    start_return(tp)

    @pl.when(tp == 0)
    def _():
        rin[...] = jnp.zeros_like(rin)

    @pl.when(tp == tp_count - 1)
    def _():
        lin[...] = jnp.zeros_like(lin)

    def mixing(block):
        slot_ids = lax.broadcasted_iota(jnp.int32, (slots, rows), 0).astype(jnp.float32)
        parts = []
        for d in range(ep_count):
            expert = lax.rem(ep + ep_count - d, ep_count) * tp_count + tp
            places = metag[block, pl.ds(expert, 1), :]
            scales = metag[block, pl.ds(experts + expert, 1), :]
            parts.append(jnp.where(slot_ids == places, scales, 0.0))
        weights = jnp.concatenate(parts, axis=0)
        high = weights.astype(jnp.bfloat16)
        low = (weights - high.astype(jnp.float32)).astype(jnp.bfloat16)
        return high, low

    def partial(block, high, low, span):
        picked = back[block, :, span]
        turned = (((0,), (0,)), ((), ()))
        return (
            lax.dot_general(high, picked, turned, preferred_element_type=jnp.float32)
            + lax.dot_general(low, picked, turned, preferred_element_type=jnp.float32)
            + jnp.dot(hidden[block], down[:, span], preferred_element_type=jnp.float32)
        )

    def reduce_step(k, carry):
        for side in range(2):
            block = tp_count - 1 - k if side == 0 else k
            active = block > tp if side == 0 else block < tp
            arrived = rin if side == 0 else lin

            @pl.when(active)
            def _():
                wait_return(block)

                @pl.when(tp > 0 if side == 0 else tp < tp_count - 1)
                def _():
                    pass_on(side, block).wait_recv()

                high, low = mixing(block)

                def columns(c, inner):
                    span = pl.ds(pl.multiple_of(c * CHUNK, CHUNK), CHUNK)
                    psend[block, :, span] = (
                        partial(block, high, low, span) + arrived[block, :, span].astype(jnp.float32)
                    ).astype(jnp.bfloat16)
                    return inner

                lax.fori_loop(0, width // CHUNK, columns, 0)
                pass_on(side, block).start()

        return carry

    lax.fori_loop(0, tp_count - 1, reduce_step, 0)
    wait_return(tp)

    @pl.when(tp > 0)
    def _():
        pass_on(0, tp).wait_recv()

    @pl.when(tp < tp_count - 1)
    def _():
        pass_on(1, tp).wait_recv()

    high, low = mixing(tp)

    def columns(c, carry):
        span = pl.ds(pl.multiple_of(c * CHUNK, CHUNK), CHUNK)
        out[:, span] = (
            partial(tp, high, low, span)
            + rin[tp, :, span].astype(jnp.float32)
            + lin[tp, :, span].astype(jnp.float32)
        ).astype(jnp.bfloat16)
        return carry

    lax.fori_loop(0, width // CHUNK, columns, 0)

    def finish(block, carry):
        for d in range(1, ep_count):
            return_copy(block, d).wait_send()

        @pl.when(block > tp)
        def _():
            pass_on(0, block).wait_send()

        @pl.when(block < tp)
        def _():
            pass_on(1, block).wait_send()

        return carry

    lax.fori_loop(0, tp_count, finish, 0)


def combine(results, hidden, down, metag):
    ep_count, tp_count, slots, width = results.shape
    rows = hidden.shape[1]
    vmem = pl.BlockSpec(memory_space=pltpu.VMEM)
    dma = pltpu.SemaphoreType.DMA
    return pl.pallas_call(
        functools.partial(combine_kernel, ep_count, tp_count),
        out_shape=jax.ShapeDtypeStruct((rows, width), jnp.bfloat16),
        in_specs=[vmem] * 4,
        out_specs=vmem,
        scratch_shapes=[
            pltpu.VMEM((tp_count, ep_count * slots, width), jnp.bfloat16),
            pltpu.VMEM((tp_count, rows, width), jnp.bfloat16),
            pltpu.VMEM((tp_count, rows, width), jnp.bfloat16),
            pltpu.VMEM((tp_count, rows, width), jnp.bfloat16),
            dma((tp_count, ep_count)),
            dma((tp_count, ep_count)),
            dma((tp_count,)),
            dma((tp_count,)),
            dma((tp_count,)),
            dma((tp_count,)),
        ],
        compiler_params=pltpu.CompilerParams(
            collective_id=1, has_side_effects=True, vmem_limit_bytes=VMEM_LIMIT
        ),
        name="combine",
    )(results, hidden, down, metag)


def body(
    mixer_in,
    mixer_gain,
    w_query,
    w_key,
    w_value,
    sink_logit,
    moe_in,
    moe_gain,
    router,
    routes,
    expert_gate,
    expert_up,
    expert_down,
    shared_gate,
    shared_up,
    shared_down,
):
    tokens = mixer_in.shape[0]
    ep_count, tp_count = lax.axis_size("ep"), lax.axis_size("tp")
    top_count = routes.shape[1]
    experts = router.shape[1]
    capacity = 3 * top_count * tokens // (2 * experts)
    slots = -(-capacity // 16) * 16
    normed_second = rms_rows(moe_in, moe_gain)
    normed_first = rms_rows(mixer_in, mixer_gain)
    affinity = jax.nn.sigmoid(jnp.dot(normed_second, router, preferred_element_type=jnp.float32))
    hits = jnp.any(
        routes[:, :, None] == jnp.arange(experts, dtype=jnp.int32)[None, None, :], axis=1
    )
    chosen = jnp.where(hits, affinity, 0.0)
    route_weight = ROUTED_SCALE * chosen / jnp.sum(chosen, axis=-1, keepdims=True)
    earlier = jnp.tril(jnp.ones((tokens, tokens), jnp.bfloat16), -1)
    before = jnp.dot(earlier, hits.astype(jnp.bfloat16), preferred_element_type=jnp.float32)
    places = jnp.where(hits, before, -1.0)
    meta = jnp.concatenate([places, route_weight], axis=1).T
    gathered_second, gathered_first, metag, arrived = dispatch(
        normed_second, normed_first, meta, ep_count, tp_count, slots
    )
    width = normed_second.shape[1]
    flat_rows = arrived.reshape(-1, width)
    hidden_rows = (
        jax.nn.silu(jnp.dot(flat_rows, expert_gate[0], preferred_element_type=jnp.float32))
        * jnp.dot(flat_rows, expert_up[0], preferred_element_type=jnp.float32)
    ).astype(jnp.bfloat16)
    results = (
        jnp.dot(hidden_rows, expert_down[0], preferred_element_type=jnp.float32)
        .astype(jnp.bfloat16)
        .reshape(arrived.shape)
    )
    row_block = gathered_second.reshape(-1, width)
    hidden = (
        jax.nn.silu(jnp.dot(row_block, shared_gate, preferred_element_type=jnp.float32))
        * jnp.dot(row_block, shared_up, preferred_element_type=jnp.float32)
    ).astype(jnp.bfloat16)
    moe_out = combine(results, hidden.reshape(tp_count, tokens, -1), shared_down, metag)
    query_cols = w_query.shape[1]
    key_cols = w_key.shape[1]
    joined = jnp.concatenate([w_query, w_key, w_value], axis=1)
    projected = jnp.dot(
        gathered_first.reshape(-1, width), joined, preferred_element_type=jnp.float32
    )
    span_rows = projected.shape[0]
    offset = lax.axis_index("ep") * span_rows
    seq_length = span_rows * ep_count
    positions = offset + jnp.arange(span_rows, dtype=jnp.int32)
    query_rows = rotate(
        projected[:, :query_cols].reshape(span_rows, -1, HEAD_DIM), positions
    ).astype(jnp.bfloat16)
    key_rows = rotate(
        projected[:, query_cols : query_cols + key_cols].reshape(span_rows, -1, HEAD_DIM), positions
    ).astype(jnp.bfloat16)
    value_rows = projected[:, query_cols + key_cols :].astype(jnp.bfloat16)
    stacked = jnp.concatenate([key_rows.reshape(span_rows, key_cols), value_rows], axis=1)
    padded = extended(stacked, (("ep", 0),), WINDOW)
    mixed = attend(query_rows, padded, sink_logit, offset, seq_length)
    return (mixed, moe_out)


def solution(mesh):
    return jax.shard_map(
        body,
        mesh=mesh,
        in_specs=(
            P(("grp", "ep", "tp"), None),
            P(),
            P(None, "tp"),
            P(None, "tp"),
            P(None, "tp"),
            P("tp"),
            P(("grp", "ep", "tp"), None),
            P(),
            P(),
            P(("grp", "ep", "tp"), None),
            P(("ep", "tp"), None, None),
            P(("ep", "tp"), None, None),
            P(("ep", "tp"), None, None),
            P(None, "tp"),
            P(None, "tp"),
            P("tp", None),
        ),
        out_specs=(P(("grp", "ep"), "tp"), P(("grp", "ep", "tp"), None)),
        check_vma=False,
    )
```

```python
import functools

import jax
import jax.numpy as jnp
from jax import lax
from jax.experimental import pallas as pl
from jax.experimental.pallas import tpu as pltpu
from jax.sharding import PartitionSpec as P

HEAD_DIM = 64
WINDOW = 128


EPS = 1e-06
THETA = 10000.0
ROUTED_SCALE = 2.5


def extended(block, sides, width):
    for axis, dim in sides:
        count = lax.axis_size(axis)
        forward = [(i, i + 1) for i in range(count - 1)]
        backward = [(target, source) for source, target in forward]
        low = lax.ppermute(
            lax.slice_in_dim(block, block.shape[dim] - width, None, axis=dim), axis, forward
        )
        high = lax.ppermute(lax.slice_in_dim(block, 0, width, axis=dim), axis, backward)
        block = jnp.concatenate([low, block, high], axis=dim)
    return block


def rms_rows(row_block, gain_vector):
    values = row_block.astype(jnp.float32)
    factor = lax.rsqrt(jnp.mean(values * values, axis=-1, keepdims=True) + EPS)
    return (values * factor * gain_vector).astype(jnp.bfloat16)


def rotate(head_rows, positions):
    half_width = head_rows.shape[-1] // 2
    inverse = THETA ** (-(jnp.arange(half_width, dtype=jnp.float32) * 2.0) / head_rows.shape[-1])
    angles = positions.astype(jnp.float32)[:, None] * inverse[None, :]
    cosine_table = jnp.cos(angles)[:, None, :]
    sine_table = jnp.sin(angles)[:, None, :]
    first_half = head_rows[..., :half_width]
    second_half = head_rows[..., half_width:]
    return jnp.concatenate(
        [
            first_half * cosine_table - second_half * sine_table,
            second_half * cosine_table + first_half * sine_table,
        ],
        axis=-1,
    )


def attend(query_rows, stacked, sink_logit, offset, seq_length):
    span_rows, head_count, head_width = query_rows.shape
    kv_local = stacked.shape[1] // (2 * head_width)
    group_size = head_count // kv_local
    key_table = stacked[:, : kv_local * head_width].reshape(-1, kv_local, head_width)
    value_table = stacked[:, kv_local * head_width :].reshape(-1, kv_local, head_width)
    block_rows = 512
    grouped = query_rows.reshape(span_rows, kv_local, group_size, head_width)
    row_ids = jnp.arange(block_rows, dtype=jnp.int32)[:, None]
    col_ids = jnp.arange(block_rows + 2 * WINDOW, dtype=jnp.int32)[None, :]
    sink_table = sink_logit.reshape(kv_local, group_size)[:, :, None, None]

    def one_block(block_index):
        block_start = block_index * block_rows
        query_block = lax.dynamic_slice_in_dim(grouped, block_start, block_rows, 0)
        key_block = lax.dynamic_slice_in_dim(key_table, block_start, block_rows + 2 * WINDOW, 0)
        value_block = lax.dynamic_slice_in_dim(value_table, block_start, block_rows + 2 * WINDOW, 0)
        scores = jnp.einsum(
            "qkgd,ckd->kgqc", query_block, key_block, preferred_element_type=jnp.float32
        ) * head_width ** (-0.5)
        key_pos = offset + block_start - WINDOW + col_ids
        query_pos = offset + block_start + row_ids
        in_window = (
            (jnp.abs(key_pos - query_pos) <= WINDOW) & (key_pos >= 0) & (key_pos < seq_length)
        )
        scores = jnp.where(in_window[None, None], scores, -jnp.inf)
        row_max = jnp.maximum(jnp.max(scores, axis=-1, keepdims=True), sink_table)
        weights = jnp.exp(scores - row_max)
        denominator = jnp.sum(weights, axis=-1, keepdims=True) + jnp.exp(sink_table - row_max)
        probability = (weights / denominator).astype(jnp.bfloat16)
        output = jnp.einsum(
            "kgqc,ckd->qkgd", probability, value_block, preferred_element_type=jnp.float32
        )
        return output.reshape(block_rows, head_count * head_width).astype(jnp.bfloat16)

    blocks_out = lax.map(one_block, jnp.arange(span_rows // block_rows, dtype=jnp.int32))
    return blocks_out.reshape(span_rows, head_count * head_width)


MESH = pl.DeviceIdType.MESH
VMEM_LIMIT = 63 * 2**20
CHUNK = 512


def remote(src, dst, send_sem, recv_sem, device):
    return pltpu.make_async_remote_copy(
        src_ref=src,
        dst_ref=dst,
        send_sem=send_sem,
        recv_sem=recv_sem,
        device_id=device,
        device_id_type=MESH,
    )


def entry_barrier(grp, ep, tp, ep_count, tp_count):
    barrier = pltpu.get_barrier_semaphore()

    @pl.when(tp > 0)
    def _():
        pl.semaphore_signal(barrier, inc=1, device_id=(grp, ep, tp - 1), device_id_type=MESH)

    @pl.when(tp < tp_count - 1)
    def _():
        pl.semaphore_signal(barrier, inc=1, device_id=(grp, ep, tp + 1), device_id_type=MESH)

    for d in range(1, ep_count):
        pl.semaphore_signal(
            barrier, inc=1, device_id=(grp, lax.rem(ep + d, ep_count), tp), device_id_type=MESH
        )

    inner = (tp > 0) & (tp < tp_count - 1)
    pl.semaphore_wait(barrier, ep_count + jnp.where(inner, 1, 0))


def layer_kernel(
    ep_count, tp_count, slots,
    second, first, meta, gate_hbm, up_hbm, down_hbm, sgate, sup, sdown,
    out, gath1,
    gath2, metag, sbuf, disp, back, sides, psend, gate, up, down, hidden, hexp,
    own_sem, w_sem, s2, r2, sm, rm, s1, r1, sd, rd, sb, rb, sp, rs,
):
    grp, ep, tp = lax.axis_index("grp"), lax.axis_index("ep"), lax.axis_index("tp")
    rows, width = second.shape
    experts = meta.shape[0] // 2
    total = ep_count * slots
    entry_barrier(grp, ep, tp, ep_count, tp_count)
    own_copies = [
        pltpu.make_async_copy(second, gath2.at[tp], own_sem.at[0]),
        pltpu.make_async_copy(meta, metag.at[tp], own_sem.at[1]),
        pltpu.make_async_copy(first, gath1.at[tp], own_sem.at[2]),
    ]
    weight_copies = [
        pltpu.make_async_copy(gate_hbm.at[0], gate, w_sem.at[0]),
        pltpu.make_async_copy(up_hbm.at[0], up, w_sem.at[1]),
        pltpu.make_async_copy(down_hbm.at[0], down, w_sem.at[2]),
    ]

    def toward(side):
        return (grp, ep, tp + (1 if side == 0 else -1))

    def exists(side):
        return tp < tp_count - 1 if side == 0 else tp > 0

    def peer(d):
        return (grp, lax.rem(ep + d, ep_count), tp)

    def spans(body, size=CHUNK, extent=width):
        def step(c, carry):
            body(pl.ds(pl.multiple_of(c * size, size), size))
            return carry

        lax.fori_loop(0, extent // size, step, 0)

    def send_second(side, block, own):
        return [
            remote(second if own else gath2.at[block], gath2.at[block], s2.at[side, block], r2.at[block], toward(side)),
            remote(meta if own else metag.at[block], metag.at[block], sm.at[side, block], rm.at[block], toward(side)),
        ]

    def send_first(side, block, own):
        return remote(first if own else gath1.at[block], gath1.at[block], s1.at[side, block], r1.at[block], toward(side))

    def start_own_first(side, step):
        last = tp if side == 0 else tp_count - 1 - tp

        @pl.when(exists(side) & (step == last))
        def _():
            send_first(side, tp, True).start()

    def dispatch_copy(block, d):
        part = pl.ds(d * slots, slots)
        return remote(sbuf.at[block, part], disp.at[block, part], sd.at[block, d], rd.at[block, d], peer(d))

    def return_copy(block, d):
        part = pl.ds(d * slots, slots)
        return remote(sbuf.at[block, part], back.at[block, part], sb.at[block, d], rb.at[block, d], peer(ep_count - d))

    def pass_on(side, block):
        return remote(psend.at[block], sides.at[side, block], sp.at[block], rs.at[side, block], toward(side))

    def places_of(block, d):
        expert = lax.rem(ep + d, ep_count) * tp_count + tp
        slot_ids = lax.broadcasted_iota(jnp.int32, (slots, rows), 0).astype(jnp.float32)
        return slot_ids == metag[block, pl.ds(expert, 1), :], expert

    def process(block):
        picks = [jnp.where(places_of(block, d)[0], 1.0, 0.0) for d in range(ep_count)]
        pick = jnp.concatenate(picks, axis=0).astype(jnp.bfloat16)

        def columns(span):
            picked = jnp.dot(pick, gath2[block, :, span], preferred_element_type=jnp.float32).astype(jnp.bfloat16)
            disp[block, 0:slots, span] = picked[0:slots]
            sbuf[block, slots:total, span] = picked[slots:total]

        spans(columns)
        for d in range(1, ep_count):
            dispatch_copy(block, d).start()

    def shared_hidden(block):
        values = gath2[block]
        gated = jnp.dot(values, sgate[...], preferred_element_type=jnp.float32)
        lifted = jnp.dot(values, sup[...], preferred_element_type=jnp.float32)
        hidden[block] = (jax.nn.silu(gated) * lifted).astype(jnp.bfloat16)

    def expert(block):
        for d in range(1, ep_count):
            dispatch_copy(block, d).wait()

        def units(span):
            values = disp[block]
            gated = jnp.dot(values, gate[:, span], preferred_element_type=jnp.float32)
            lifted = jnp.dot(values, up[:, span], preferred_element_type=jnp.float32)
            hexp[:, span] = (jax.nn.silu(gated) * lifted).astype(jnp.bfloat16)

        spans(units, 256, gate.shape[1])

        def columns(span):
            result = jnp.dot(hexp[...], down[:, span], preferred_element_type=jnp.float32).astype(jnp.bfloat16)
            back[block, 0:slots, span] = result[0:slots]
            sbuf[block, slots:total, span] = result[slots:total]

        spans(columns)
        for d in range(1, ep_count):
            return_copy(block, d).start()

    def experts_at(distance):
        def one(side, carry):
            block = tp + (2 * side - 1) * distance

            @pl.when((block >= 0) & (block < tp_count) & ((distance > 0) | (side == 0)))
            def _():
                expert(block)

            return carry

        lax.fori_loop(0, 2, one, 0)

    for side in range(2):

        @pl.when(exists(side))
        def _():
            for copy in send_second(side, tp, True):
                copy.start()

        start_own_first(side, 0)
    for copy in own_copies + weight_copies:
        copy.start()

    @pl.when(tp == 0)
    def _():
        sides[0] = jnp.zeros(sides.shape[1:], sides.dtype)

    @pl.when(tp == tp_count - 1)
    def _():
        sides[1] = jnp.zeros(sides.shape[1:], sides.dtype)

    own_copies[0].wait()
    own_copies[1].wait()
    process(tp)
    shared_hidden(tp)
    for copy in weight_copies:
        copy.wait()

    def hop(k, carry):
        for side in range(2):
            block = tp - k if side == 0 else tp + k
            inside = block >= 0 if side == 0 else block < tp_count

            @pl.when(inside)
            def _():
                for copy in send_second(side, block, False):
                    copy.wait_recv()

                @pl.when(exists(side))
                def _():
                    for copy in send_second(side, block, False):
                        copy.start()

            start_own_first(side, k)

            @pl.when(inside)
            def _():
                process(block)
                shared_hidden(block)

        experts_at(k - 1)
        return carry

    lax.fori_loop(1, tp_count, hop, 0)
    own_copies[2].wait()

    def partial_of(block):
        parts = []
        for d in range(ep_count):
            hit, number = places_of(block, d)
            parts.append(jnp.where(hit, metag[block, pl.ds(experts + number, 1), :], 0.0))
        weights = jnp.concatenate(parts, axis=0)
        high = weights.astype(jnp.bfloat16)
        low = (weights - high.astype(jnp.float32)).astype(jnp.bfloat16)
        turned = (((0,), (0,)), ((), ()))

        def value(span):
            picked = back[block, :, span]
            return (
                lax.dot_general(high, picked, turned, preferred_element_type=jnp.float32)
                + lax.dot_general(low, picked, turned, preferred_element_type=jnp.float32)
                + jnp.dot(hidden[block], sdown[:, span], preferred_element_type=jnp.float32)
            )

        return value

    def wait_return(block):
        for d in range(1, ep_count):
            return_copy(block, d).wait_recv()

    def reduce_step(k):
        for side in range(2):
            block = tp_count - 1 - k if side == 0 else k
            active = block > tp if side == 0 else block < tp

            @pl.when(active)
            def _():
                wait_return(block)

                @pl.when(tp > 0 if side == 0 else tp < tp_count - 1)
                def _():
                    pass_on(side, block).wait_recv()

                value = partial_of(block)

                def columns(span):
                    psend[block, :, span] = (
                        value(span) + sides[side, block, :, span].astype(jnp.float32)
                    ).astype(jnp.bfloat16)

                spans(columns)
                pass_on(side, block).start()

    def hop_first(k, carry):
        for side in range(2):
            block = tp - k if side == 0 else tp + k
            inside = block >= 0 if side == 0 else block < tp_count

            @pl.when(inside)
            def _():
                send_first(side, block, False).wait_recv()

                @pl.when(exists(side))
                def _():
                    send_first(side, block, False).start()

        @pl.when(k == 1)
        def _():
            experts_at(tp_count - 1)

        @pl.when(k > 1)
        def _():
            reduce_step(k - 2)

        return carry

    lax.fori_loop(1, tp_count, hop_first, 0)
    reduce_step(tp_count - 2)
    wait_return(tp)

    @pl.when(tp > 0)
    def _():
        pass_on(0, tp).wait_recv()

    @pl.when(tp < tp_count - 1)
    def _():
        pass_on(1, tp).wait_recv()

    own_value = partial_of(tp)

    def columns(span):
        out[:, span] = (
            own_value(span)
            + sides[0, tp, :, span].astype(jnp.float32)
            + sides[1, tp, :, span].astype(jnp.float32)
        ).astype(jnp.bfloat16)

    spans(columns)

    def finish(block, carry):
        for d in range(1, ep_count):
            return_copy(block, d).wait_send()
        for side in range(2):
            passed = block <= tp if side == 0 else block >= tp
            summed = block > tp if side == 0 else block < tp

            @pl.when(exists(side) & passed)
            def _():
                for copy in send_second(side, block, False):
                    copy.wait_send()
                send_first(side, block, False).wait_send()

            @pl.when(summed)
            def _():
                pass_on(side, block).wait_send()

        return carry

    lax.fori_loop(0, tp_count, finish, 0)


def layer(second, first, meta, gate, up, down, sgate, sup, sdown, ep_count, tp_count, slots):
    rows, width = second.shape
    vmem = pl.BlockSpec(memory_space=pltpu.VMEM)
    hbm = pl.BlockSpec(memory_space=pl.ANY)
    dma = pltpu.SemaphoreType.DMA
    bf16 = jnp.bfloat16
    total = ep_count * slots
    return pl.pallas_call(
        functools.partial(layer_kernel, ep_count, tp_count, slots),
        out_shape=(
            jax.ShapeDtypeStruct((rows, width), bf16),
            jax.ShapeDtypeStruct((tp_count, rows, width), bf16),
        ),
        in_specs=[vmem] * 3 + [hbm] * 3 + [vmem] * 3,
        out_specs=(vmem, vmem),
        scratch_shapes=[
            pltpu.VMEM((tp_count, rows, width), bf16),
            pltpu.VMEM((tp_count,) + meta.shape, jnp.float32),
            pltpu.VMEM((tp_count, total, width), bf16),
            pltpu.VMEM((tp_count, total, width), bf16),
            pltpu.VMEM((tp_count, total, width), bf16),
            pltpu.VMEM((2, tp_count, rows, width), bf16),
            pltpu.VMEM((tp_count, rows, width), bf16),
            pltpu.VMEM(gate.shape[1:], bf16),
            pltpu.VMEM(up.shape[1:], bf16),
            pltpu.VMEM(down.shape[1:], bf16),
            pltpu.VMEM((tp_count, rows, sgate.shape[1]), bf16),
            pltpu.VMEM((total, gate.shape[2]), bf16),
            dma((3,)),
            dma((3,)),
            dma((2, tp_count)),
            dma((tp_count,)),
            dma((2, tp_count)),
            dma((tp_count,)),
            dma((2, tp_count)),
            dma((tp_count,)),
            dma((tp_count, ep_count)),
            dma((tp_count, ep_count)),
            dma((tp_count, ep_count)),
            dma((tp_count, ep_count)),
            dma((tp_count,)),
            dma((2, tp_count)),
        ],
        compiler_params=pltpu.CompilerParams(
            collective_id=0, has_side_effects=True, vmem_limit_bytes=VMEM_LIMIT
        ),
        name="layer",
    )(second, first, meta, gate, up, down, sgate, sup, sdown)


def body(
    mixer_in,
    mixer_gain,
    w_query,
    w_key,
    w_value,
    sink_logit,
    moe_in,
    moe_gain,
    router,
    routes,
    expert_gate,
    expert_up,
    expert_down,
    shared_gate,
    shared_up,
    shared_down,
):
    tokens = mixer_in.shape[0]
    ep_count, tp_count = lax.axis_size("ep"), lax.axis_size("tp")
    top_count = routes.shape[1]
    experts = router.shape[1]
    capacity = 3 * top_count * tokens // (2 * experts)
    slots = -(-capacity // 16) * 16
    normed_second = rms_rows(moe_in, moe_gain)
    normed_first = rms_rows(mixer_in, mixer_gain)
    affinity = jax.nn.sigmoid(jnp.dot(normed_second, router, preferred_element_type=jnp.float32))
    hits = jnp.any(
        routes[:, :, None] == jnp.arange(experts, dtype=jnp.int32)[None, None, :], axis=1
    )
    chosen = jnp.where(hits, affinity, 0.0)
    route_weight = ROUTED_SCALE * chosen / jnp.sum(chosen, axis=-1, keepdims=True)
    earlier = jnp.tril(jnp.ones((tokens, tokens), jnp.bfloat16), -1)
    before = jnp.dot(earlier, hits.astype(jnp.bfloat16), preferred_element_type=jnp.float32)
    places = jnp.where(hits, before, -1.0)
    meta = jnp.concatenate([places, route_weight], axis=1).T
    width = normed_second.shape[1]
    moe_out, gathered_first = layer(
        normed_second, normed_first, meta, expert_gate, expert_up, expert_down,
        shared_gate, shared_up, shared_down, ep_count, tp_count, slots,
    )
    query_cols = w_query.shape[1]
    key_cols = w_key.shape[1]
    joined = jnp.concatenate([w_query, w_key, w_value], axis=1)
    projected = jnp.dot(
        gathered_first.reshape(-1, width), joined, preferred_element_type=jnp.float32
    )
    span_rows = projected.shape[0]
    offset = lax.axis_index("ep") * span_rows
    seq_length = span_rows * ep_count
    positions = offset + jnp.arange(span_rows, dtype=jnp.int32)
    query_rows = rotate(
        projected[:, :query_cols].reshape(span_rows, -1, HEAD_DIM), positions
    ).astype(jnp.bfloat16)
    key_rows = rotate(
        projected[:, query_cols : query_cols + key_cols].reshape(span_rows, -1, HEAD_DIM), positions
    ).astype(jnp.bfloat16)
    value_rows = projected[:, query_cols + key_cols :].astype(jnp.bfloat16)
    stacked = jnp.concatenate([key_rows.reshape(span_rows, key_cols), value_rows], axis=1)
    padded = extended(stacked, (("ep", 0),), WINDOW)
    mixed = attend(query_rows, padded, sink_logit, offset, seq_length)
    return (mixed, moe_out)


def solution(mesh):
    return jax.shard_map(
        body,
        mesh=mesh,
        in_specs=(
            P(("grp", "ep", "tp"), None),
            P(),
            P(None, "tp"),
            P(None, "tp"),
            P(None, "tp"),
            P("tp"),
            P(("grp", "ep", "tp"), None),
            P(),
            P(),
            P(("grp", "ep", "tp"), None),
            P(("ep", "tp"), None, None),
            P(("ep", "tp"), None, None),
            P(("ep", "tp"), None, None),
            P(None, "tp"),
            P(None, "tp"),
            P("tp", None),
        ),
        out_specs=(P(("grp", "ep"), "tp"), P(("grp", "ep", "tp"), None)),
        check_vma=False,
    )
```

```python
import functools

import jax
import jax.numpy as jnp
from jax import lax
from jax.experimental import pallas as pl
from jax.experimental.pallas import tpu as pltpu
from jax.sharding import PartitionSpec as P

HEAD_DIM = 64
WINDOW = 128


EPS = 1e-06
THETA = 10000.0
ROUTED_SCALE = 2.5


def extended(block, sides, width):
    for axis, dim in sides:
        count = lax.axis_size(axis)
        forward = [(i, i + 1) for i in range(count - 1)]
        backward = [(target, source) for source, target in forward]
        low = lax.ppermute(
            lax.slice_in_dim(block, block.shape[dim] - width, None, axis=dim), axis, forward
        )
        high = lax.ppermute(lax.slice_in_dim(block, 0, width, axis=dim), axis, backward)
        block = jnp.concatenate([low, block, high], axis=dim)
    return block


def rms_rows(row_block, gain_vector):
    values = row_block.astype(jnp.float32)
    factor = lax.rsqrt(jnp.mean(values * values, axis=-1, keepdims=True) + EPS)
    return (values * factor * gain_vector).astype(jnp.bfloat16)


def rotate(head_rows, positions):
    half_width = head_rows.shape[-1] // 2
    inverse = THETA ** (-(jnp.arange(half_width, dtype=jnp.float32) * 2.0) / head_rows.shape[-1])
    angles = positions.astype(jnp.float32)[:, None] * inverse[None, :]
    cosine_table = jnp.cos(angles)[:, None, :]
    sine_table = jnp.sin(angles)[:, None, :]
    first_half = head_rows[..., :half_width]
    second_half = head_rows[..., half_width:]
    return jnp.concatenate(
        [
            first_half * cosine_table - second_half * sine_table,
            second_half * cosine_table + first_half * sine_table,
        ],
        axis=-1,
    )


def attend(query_rows, stacked, sink_logit, offset, seq_length):
    span_rows, head_count, head_width = query_rows.shape
    kv_local = stacked.shape[1] // (2 * head_width)
    group_size = head_count // kv_local
    key_table = stacked[:, : kv_local * head_width].reshape(-1, kv_local, head_width)
    value_table = stacked[:, kv_local * head_width :].reshape(-1, kv_local, head_width)
    block_rows = 512
    grouped = query_rows.reshape(span_rows, kv_local, group_size, head_width)
    row_ids = jnp.arange(block_rows, dtype=jnp.int32)[:, None]
    col_ids = jnp.arange(block_rows + 2 * WINDOW, dtype=jnp.int32)[None, :]
    sink_table = sink_logit.reshape(kv_local, group_size)[:, :, None, None]

    def one_block(block_index):
        block_start = block_index * block_rows
        query_block = lax.dynamic_slice_in_dim(grouped, block_start, block_rows, 0)
        key_block = lax.dynamic_slice_in_dim(key_table, block_start, block_rows + 2 * WINDOW, 0)
        value_block = lax.dynamic_slice_in_dim(value_table, block_start, block_rows + 2 * WINDOW, 0)
        scores = jnp.einsum(
            "qkgd,ckd->kgqc", query_block, key_block, preferred_element_type=jnp.float32
        ) * head_width ** (-0.5)
        key_pos = offset + block_start - WINDOW + col_ids
        query_pos = offset + block_start + row_ids
        in_window = (
            (jnp.abs(key_pos - query_pos) <= WINDOW) & (key_pos >= 0) & (key_pos < seq_length)
        )
        scores = jnp.where(in_window[None, None], scores, -jnp.inf)
        row_max = jnp.maximum(jnp.max(scores, axis=-1, keepdims=True), sink_table)
        weights = jnp.exp(scores - row_max)
        denominator = jnp.sum(weights, axis=-1, keepdims=True) + jnp.exp(sink_table - row_max)
        probability = (weights / denominator).astype(jnp.bfloat16)
        output = jnp.einsum(
            "kgqc,ckd->qkgd", probability, value_block, preferred_element_type=jnp.float32
        )
        return output.reshape(block_rows, head_count * head_width).astype(jnp.bfloat16)

    blocks_out = lax.map(one_block, jnp.arange(span_rows // block_rows, dtype=jnp.int32))
    return blocks_out.reshape(span_rows, head_count * head_width)


MESH = pl.DeviceIdType.MESH
VMEM_LIMIT = 63 * 2**20
CHUNK = 512


def remote(src, dst, send_sem, recv_sem, device):
    return pltpu.make_async_remote_copy(
        src_ref=src,
        dst_ref=dst,
        send_sem=send_sem,
        recv_sem=recv_sem,
        device_id=device,
        device_id_type=MESH,
    )


def entry_barrier(grp, ep, tp, ep_count, tp_count):
    barrier = pltpu.get_barrier_semaphore()

    @pl.when(tp > 0)
    def _():
        pl.semaphore_signal(barrier, inc=1, device_id=(grp, ep, tp - 1), device_id_type=MESH)

    @pl.when(tp < tp_count - 1)
    def _():
        pl.semaphore_signal(barrier, inc=1, device_id=(grp, ep, tp + 1), device_id_type=MESH)

    for d in range(1, ep_count):
        pl.semaphore_signal(
            barrier, inc=1, device_id=(grp, lax.rem(ep + d, ep_count), tp), device_id_type=MESH
        )

    inner = (tp > 0) & (tp < tp_count - 1)
    pl.semaphore_wait(barrier, ep_count + jnp.where(inner, 1, 0))


def layer_kernel(
    ep_count, tp_count, slots,
    second, first, meta, gate_hbm, up_hbm, down_hbm, sgate, sup, sdown,
    out, gath1,
    gath2, metag, sbuf, disp, back, sides, psend, gate, up, down, hidden, hexp,
    own_sem, w_sem, s2, r2, sm, rm, s1, r1, sd, rd, sb, rb, sp, rs,
):
    grp, ep, tp = lax.axis_index("grp"), lax.axis_index("ep"), lax.axis_index("tp")
    rows, width = second.shape
    experts = meta.shape[0] // 2
    total = ep_count * slots
    entry_barrier(grp, ep, tp, ep_count, tp_count)
    own_copies = [
        pltpu.make_async_copy(second, gath2.at[tp], own_sem.at[0]),
        pltpu.make_async_copy(meta, metag.at[tp], own_sem.at[1]),
        pltpu.make_async_copy(first, gath1.at[tp], own_sem.at[2]),
    ]
    weight_copies = [
        pltpu.make_async_copy(gate_hbm.at[0], gate, w_sem.at[0]),
        pltpu.make_async_copy(up_hbm.at[0], up, w_sem.at[1]),
        pltpu.make_async_copy(down_hbm.at[0], down, w_sem.at[2]),
    ]

    def toward(side):
        return (grp, ep, tp + (1 if side == 0 else -1))

    def exists(side):
        return tp < tp_count - 1 if side == 0 else tp > 0

    def peer(d):
        return (grp, lax.rem(ep + d, ep_count), tp)

    def spans(body, size=CHUNK, extent=width):
        def step(c, carry):
            body(pl.ds(pl.multiple_of(c * size, size), size))
            return carry

        lax.fori_loop(0, extent // size, step, 0)

    def send_second(side, block, own):
        return [
            remote(second if own else gath2.at[block], gath2.at[block], s2.at[side, block], r2.at[block], toward(side)),
            remote(meta if own else metag.at[block], metag.at[block], sm.at[side, block], rm.at[block], toward(side)),
        ]

    def send_first(side, block, own):
        return remote(first if own else gath1.at[block], gath1.at[block], s1.at[side, block], r1.at[block], toward(side))

    def start_own_first(side, step):
        last = tp if side == 0 else tp_count - 1 - tp

        @pl.when(exists(side) & (step == last))
        def _():
            send_first(side, tp, True).start()

    def dispatch_copy(block, d):
        part = pl.ds(d * slots, slots)
        return remote(sbuf.at[block, part], disp.at[block, part], sd.at[block, d], rd.at[block, d], peer(d))

    def return_copy(block, d):
        part = pl.ds(d * slots, slots)
        return remote(sbuf.at[block, part], back.at[block, part], sb.at[block, d], rb.at[block, d], peer(ep_count - d))

    parts = width // CHUNK

    def part_span(part):
        return pl.ds(pl.multiple_of(part * CHUNK, CHUNK), CHUNK)

    def pass_on(side, block, part):
        span = part_span(part)
        return remote(
            psend.at[block, :, span], sides.at[side, block, :, span],
            sp.at[block, part], rs.at[side, block, part], toward(side),
        )

    def places_of(block, d):
        expert = lax.rem(ep + d, ep_count) * tp_count + tp
        slot_ids = lax.broadcasted_iota(jnp.int32, (slots, rows), 0).astype(jnp.float32)
        return slot_ids == metag[block, pl.ds(expert, 1), :], expert

    def process(block):
        picks = [jnp.where(places_of(block, d)[0], 1.0, 0.0) for d in range(ep_count)]
        pick = jnp.concatenate(picks, axis=0).astype(jnp.bfloat16)

        def columns(span):
            picked = jnp.dot(pick, gath2[block, :, span], preferred_element_type=jnp.float32).astype(jnp.bfloat16)
            disp[block, 0:slots, span] = picked[0:slots]
            sbuf[block, slots:total, span] = picked[slots:total]

        spans(columns)
        for d in range(1, ep_count):
            dispatch_copy(block, d).start()

    def shared_hidden(block):
        values = gath2[block]
        gated = jnp.dot(values, sgate[...], preferred_element_type=jnp.float32)
        lifted = jnp.dot(values, sup[...], preferred_element_type=jnp.float32)
        hidden[block] = (jax.nn.silu(gated) * lifted).astype(jnp.bfloat16)

    def expert(block):
        for d in range(1, ep_count):
            dispatch_copy(block, d).wait()

        def units(span):
            values = disp[block]
            gated = jnp.dot(values, gate[:, span], preferred_element_type=jnp.float32)
            lifted = jnp.dot(values, up[:, span], preferred_element_type=jnp.float32)
            hexp[:, span] = (jax.nn.silu(gated) * lifted).astype(jnp.bfloat16)

        spans(units, 256, gate.shape[1])

        def columns(span):
            result = jnp.dot(hexp[...], down[:, span], preferred_element_type=jnp.float32).astype(jnp.bfloat16)
            back[block, 0:slots, span] = result[0:slots]
            sbuf[block, slots:total, span] = result[slots:total]

        spans(columns)
        for d in range(1, ep_count):
            return_copy(block, d).start()

    def experts_at(distance):
        def one(side, carry):
            block = tp + (2 * side - 1) * distance

            @pl.when((block >= 0) & (block < tp_count) & ((distance > 0) | (side == 0)))
            def _():
                expert(block)

            return carry

        lax.fori_loop(0, 2, one, 0)

    for side in range(2):

        @pl.when(exists(side))
        def _():
            for copy in send_second(side, tp, True):
                copy.start()

        start_own_first(side, 0)
    for copy in own_copies + weight_copies:
        copy.start()

    @pl.when(tp == 0)
    def _():
        sides[0] = jnp.zeros(sides.shape[1:], sides.dtype)

    @pl.when(tp == tp_count - 1)
    def _():
        sides[1] = jnp.zeros(sides.shape[1:], sides.dtype)

    own_copies[0].wait()
    own_copies[1].wait()
    process(tp)
    shared_hidden(tp)
    for copy in weight_copies:
        copy.wait()

    def hop(k, carry):
        for side in range(2):
            block = tp - k if side == 0 else tp + k
            inside = block >= 0 if side == 0 else block < tp_count

            @pl.when(inside)
            def _():
                for copy in send_second(side, block, False):
                    copy.wait_recv()

                @pl.when(exists(side))
                def _():
                    for copy in send_second(side, block, False):
                        copy.start()

            start_own_first(side, k)

            @pl.when(inside)
            def _():
                process(block)
                shared_hidden(block)

        experts_at(k - 1)
        return carry

    lax.fori_loop(1, tp_count, hop, 0)
    own_copies[2].wait()

    def partial_of(block):
        pieces = []
        for d in range(ep_count):
            hit, number = places_of(block, d)
            pieces.append(jnp.where(hit, metag[block, pl.ds(experts + number, 1), :], 0.0))
        weights = jnp.concatenate(pieces, axis=0)
        high = weights.astype(jnp.bfloat16)
        low = (weights - high.astype(jnp.float32)).astype(jnp.bfloat16)
        turned = (((0,), (0,)), ((), ()))

        def value(span):
            picked = back[block, :, span]
            return (
                lax.dot_general(high, picked, turned, preferred_element_type=jnp.float32)
                + lax.dot_general(low, picked, turned, preferred_element_type=jnp.float32)
                + jnp.dot(hidden[block], sdown[:, span], preferred_element_type=jnp.float32)
            )

        return value

    def wait_return(block):
        for d in range(1, ep_count):
            return_copy(block, d).wait_recv()

    def reduce_step(step):
        for side in range(2):
            block = step - tp if side == 0 else 2 * (tp_count - 1) - step - tp
            active = (block > tp) & (block < tp_count) if side == 0 else (block < tp) & (block >= 0)

            @pl.when(active)
            def _():
                wait_return(block)
                value = partial_of(block)

                def one_part(part, carry):
                    span = part_span(part)
                    own = value(span)

                    @pl.when(tp > 0 if side == 0 else tp < tp_count - 1)
                    def _():
                        pass_on(side, block, part).wait_recv()

                    psend[block, :, span] = (
                        own + sides[side, block, :, span].astype(jnp.float32)
                    ).astype(jnp.bfloat16)
                    pass_on(side, block, part).start()
                    return carry

                lax.fori_loop(0, parts, one_part, 0)

    def hop_first(k, carry):
        for side in range(2):
            block = tp - k if side == 0 else tp + k
            inside = block >= 0 if side == 0 else block < tp_count

            @pl.when(inside)
            def _():
                send_first(side, block, False).wait_recv()

                @pl.when(exists(side))
                def _():
                    send_first(side, block, False).start()

        @pl.when(k == 1)
        def _():
            experts_at(tp_count - 1)

        reduce_step(2 * k - 1)
        reduce_step(2 * k)
        return carry

    lax.fori_loop(1, tp_count, hop_first, 0)
    wait_return(tp)
    own_value = partial_of(tp)

    def last_part(part, carry):
        span = part_span(part)
        own = own_value(span)

        @pl.when(tp > 0)
        def _():
            pass_on(0, tp, part).wait_recv()

        @pl.when(tp < tp_count - 1)
        def _():
            pass_on(1, tp, part).wait_recv()

        out[:, span] = (
            own
            + sides[0, tp, :, span].astype(jnp.float32)
            + sides[1, tp, :, span].astype(jnp.float32)
        ).astype(jnp.bfloat16)
        return carry

    lax.fori_loop(0, parts, last_part, 0)

    def finish(block, carry):
        for d in range(1, ep_count):
            return_copy(block, d).wait_send()
        for side in range(2):
            passed = block <= tp if side == 0 else block >= tp
            summed = block > tp if side == 0 else block < tp

            @pl.when(exists(side) & passed)
            def _():
                for copy in send_second(side, block, False):
                    copy.wait_send()
                send_first(side, block, False).wait_send()

            @pl.when(summed)
            def _():
                for part in range(parts):
                    pass_on(side, block, part).wait_send()

        return carry

    lax.fori_loop(0, tp_count, finish, 0)


def layer(second, first, meta, gate, up, down, sgate, sup, sdown, ep_count, tp_count, slots):
    rows, width = second.shape
    vmem = pl.BlockSpec(memory_space=pltpu.VMEM)
    hbm = pl.BlockSpec(memory_space=pl.ANY)
    dma = pltpu.SemaphoreType.DMA
    bf16 = jnp.bfloat16
    total = ep_count * slots
    return pl.pallas_call(
        functools.partial(layer_kernel, ep_count, tp_count, slots),
        out_shape=(
            jax.ShapeDtypeStruct((rows, width), bf16),
            jax.ShapeDtypeStruct((tp_count, rows, width), bf16),
        ),
        in_specs=[vmem] * 3 + [hbm] * 3 + [vmem] * 3,
        out_specs=(vmem, vmem),
        scratch_shapes=[
            pltpu.VMEM((tp_count, rows, width), bf16),
            pltpu.VMEM((tp_count,) + meta.shape, jnp.float32),
            pltpu.VMEM((tp_count, total, width), bf16),
            pltpu.VMEM((tp_count, total, width), bf16),
            pltpu.VMEM((tp_count, total, width), bf16),
            pltpu.VMEM((2, tp_count, rows, width), bf16),
            pltpu.VMEM((tp_count, rows, width), bf16),
            pltpu.VMEM(gate.shape[1:], bf16),
            pltpu.VMEM(up.shape[1:], bf16),
            pltpu.VMEM(down.shape[1:], bf16),
            pltpu.VMEM((tp_count, rows, sgate.shape[1]), bf16),
            pltpu.VMEM((total, gate.shape[2]), bf16),
            dma((3,)),
            dma((3,)),
            dma((2, tp_count)),
            dma((tp_count,)),
            dma((2, tp_count)),
            dma((tp_count,)),
            dma((2, tp_count)),
            dma((tp_count,)),
            dma((tp_count, ep_count)),
            dma((tp_count, ep_count)),
            dma((tp_count, ep_count)),
            dma((tp_count, ep_count)),
            dma((tp_count, width // CHUNK)),
            dma((2, tp_count, width // CHUNK)),
        ],
        compiler_params=pltpu.CompilerParams(
            collective_id=0, has_side_effects=True, vmem_limit_bytes=VMEM_LIMIT
        ),
        name="layer",
    )(second, first, meta, gate, up, down, sgate, sup, sdown)


def body(
    mixer_in,
    mixer_gain,
    w_query,
    w_key,
    w_value,
    sink_logit,
    moe_in,
    moe_gain,
    router,
    routes,
    expert_gate,
    expert_up,
    expert_down,
    shared_gate,
    shared_up,
    shared_down,
):
    tokens = mixer_in.shape[0]
    ep_count, tp_count = lax.axis_size("ep"), lax.axis_size("tp")
    top_count = routes.shape[1]
    experts = router.shape[1]
    capacity = 3 * top_count * tokens // (2 * experts)
    slots = -(-capacity // 16) * 16
    normed_second = rms_rows(moe_in, moe_gain)
    normed_first = rms_rows(mixer_in, mixer_gain)
    affinity = jax.nn.sigmoid(jnp.dot(normed_second, router, preferred_element_type=jnp.float32))
    hits = jnp.any(
        routes[:, :, None] == jnp.arange(experts, dtype=jnp.int32)[None, None, :], axis=1
    )
    chosen = jnp.where(hits, affinity, 0.0)
    route_weight = ROUTED_SCALE * chosen / jnp.sum(chosen, axis=-1, keepdims=True)
    earlier = jnp.tril(jnp.ones((tokens, tokens), jnp.bfloat16), -1)
    before = jnp.dot(earlier, hits.astype(jnp.bfloat16), preferred_element_type=jnp.float32)
    places = jnp.where(hits, before, -1.0)
    meta = jnp.concatenate([places, route_weight], axis=1).T
    width = normed_second.shape[1]
    moe_out, gathered_first = layer(
        normed_second, normed_first, meta, expert_gate, expert_up, expert_down,
        shared_gate, shared_up, shared_down, ep_count, tp_count, slots,
    )
    query_cols = w_query.shape[1]
    key_cols = w_key.shape[1]
    joined = jnp.concatenate([w_query, w_key, w_value], axis=1)
    projected = jnp.dot(
        gathered_first.reshape(-1, width), joined, preferred_element_type=jnp.float32
    )
    span_rows = projected.shape[0]
    offset = lax.axis_index("ep") * span_rows
    seq_length = span_rows * ep_count
    positions = offset + jnp.arange(span_rows, dtype=jnp.int32)
    query_rows = rotate(
        projected[:, :query_cols].reshape(span_rows, -1, HEAD_DIM), positions
    ).astype(jnp.bfloat16)
    key_rows = rotate(
        projected[:, query_cols : query_cols + key_cols].reshape(span_rows, -1, HEAD_DIM), positions
    ).astype(jnp.bfloat16)
    value_rows = projected[:, query_cols + key_cols :].astype(jnp.bfloat16)
    stacked = jnp.concatenate([key_rows.reshape(span_rows, key_cols), value_rows], axis=1)
    padded = extended(stacked, (("ep", 0),), WINDOW)
    mixed = attend(query_rows, padded, sink_logit, offset, seq_length)
    return (mixed, moe_out)


def solution(mesh):
    return jax.shard_map(
        body,
        mesh=mesh,
        in_specs=(
            P(("grp", "ep", "tp"), None),
            P(),
            P(None, "tp"),
            P(None, "tp"),
            P(None, "tp"),
            P("tp"),
            P(("grp", "ep", "tp"), None),
            P(),
            P(),
            P(("grp", "ep", "tp"), None),
            P(("ep", "tp"), None, None),
            P(("ep", "tp"), None, None),
            P(("ep", "tp"), None, None),
            P(None, "tp"),
            P(None, "tp"),
            P("tp", None),
        ),
        out_specs=(P(("grp", "ep"), "tp"), P(("grp", "ep", "tp"), None)),
        check_vma=False,
    )
```

```python
import functools

import jax
import jax.numpy as jnp
from jax import lax
from jax.experimental import pallas as pl
from jax.experimental.pallas import tpu as pltpu
from jax.sharding import PartitionSpec as P

HEAD_DIM = 64
WINDOW = 128


EPS = 1e-06
THETA = 10000.0
ROUTED_SCALE = 2.5


def extended(block, sides, width):
    for axis, dim in sides:
        count = lax.axis_size(axis)
        forward = [(i, i + 1) for i in range(count - 1)]
        backward = [(target, source) for source, target in forward]
        low = lax.ppermute(
            lax.slice_in_dim(block, block.shape[dim] - width, None, axis=dim), axis, forward
        )
        high = lax.ppermute(lax.slice_in_dim(block, 0, width, axis=dim), axis, backward)
        block = jnp.concatenate([low, block, high], axis=dim)
    return block


def rms_rows(row_block, gain_vector):
    values = row_block.astype(jnp.float32)
    factor = lax.rsqrt(jnp.mean(values * values, axis=-1, keepdims=True) + EPS)
    return (values * factor * gain_vector).astype(jnp.bfloat16)


def rotate(head_rows, positions):
    half_width = head_rows.shape[-1] // 2
    inverse = THETA ** (-(jnp.arange(half_width, dtype=jnp.float32) * 2.0) / head_rows.shape[-1])
    angles = positions.astype(jnp.float32)[:, None] * inverse[None, :]
    cosine_table = jnp.cos(angles)[:, None, :]
    sine_table = jnp.sin(angles)[:, None, :]
    first_half = head_rows[..., :half_width]
    second_half = head_rows[..., half_width:]
    return jnp.concatenate(
        [
            first_half * cosine_table - second_half * sine_table,
            second_half * cosine_table + first_half * sine_table,
        ],
        axis=-1,
    )


def attend(query_rows, stacked, sink_logit, offset, seq_length):
    span_rows, head_count, head_width = query_rows.shape
    kv_local = stacked.shape[1] // (2 * head_width)
    group_size = head_count // kv_local
    key_table = stacked[:, : kv_local * head_width].reshape(-1, kv_local, head_width)
    value_table = stacked[:, kv_local * head_width :].reshape(-1, kv_local, head_width)
    block_rows = 512
    grouped = query_rows.reshape(span_rows, kv_local, group_size, head_width)
    row_ids = jnp.arange(block_rows, dtype=jnp.int32)[:, None]
    col_ids = jnp.arange(block_rows + 2 * WINDOW, dtype=jnp.int32)[None, :]
    sink_table = sink_logit.reshape(kv_local, group_size)[:, :, None, None]

    def one_block(block_index):
        block_start = block_index * block_rows
        query_block = lax.dynamic_slice_in_dim(grouped, block_start, block_rows, 0)
        key_block = lax.dynamic_slice_in_dim(key_table, block_start, block_rows + 2 * WINDOW, 0)
        value_block = lax.dynamic_slice_in_dim(value_table, block_start, block_rows + 2 * WINDOW, 0)
        scores = jnp.einsum(
            "qkgd,ckd->kgqc", query_block, key_block, preferred_element_type=jnp.float32
        ) * head_width ** (-0.5)
        key_pos = offset + block_start - WINDOW + col_ids
        query_pos = offset + block_start + row_ids
        in_window = (
            (jnp.abs(key_pos - query_pos) <= WINDOW) & (key_pos >= 0) & (key_pos < seq_length)
        )
        scores = jnp.where(in_window[None, None], scores, -jnp.inf)
        row_max = jnp.maximum(jnp.max(scores, axis=-1, keepdims=True), sink_table)
        weights = jnp.exp(scores - row_max)
        denominator = jnp.sum(weights, axis=-1, keepdims=True) + jnp.exp(sink_table - row_max)
        probability = (weights / denominator).astype(jnp.bfloat16)
        output = jnp.einsum(
            "kgqc,ckd->qkgd", probability, value_block, preferred_element_type=jnp.float32
        )
        return output.reshape(block_rows, head_count * head_width).astype(jnp.bfloat16)

    blocks_out = lax.map(one_block, jnp.arange(span_rows // block_rows, dtype=jnp.int32))
    return blocks_out.reshape(span_rows, head_count * head_width)


MESH = pl.DeviceIdType.MESH
VMEM_LIMIT = 63 * 2**20
CHUNK = 512


def remote(src, dst, send_sem, recv_sem, device):
    return pltpu.make_async_remote_copy(
        src_ref=src,
        dst_ref=dst,
        send_sem=send_sem,
        recv_sem=recv_sem,
        device_id=device,
        device_id_type=MESH,
    )


def entry_barrier(grp, ep, tp, ep_count, tp_count):
    barrier = pltpu.get_barrier_semaphore()

    @pl.when(tp > 0)
    def _():
        pl.semaphore_signal(barrier, inc=1, device_id=(grp, ep, tp - 1), device_id_type=MESH)

    @pl.when(tp < tp_count - 1)
    def _():
        pl.semaphore_signal(barrier, inc=1, device_id=(grp, ep, tp + 1), device_id_type=MESH)

    for d in range(1, ep_count):
        pl.semaphore_signal(
            barrier, inc=1, device_id=(grp, lax.rem(ep + d, ep_count), tp), device_id_type=MESH
        )

    inner = (tp > 0) & (tp < tp_count - 1)
    pl.semaphore_wait(barrier, ep_count + jnp.where(inner, 1, 0))


def layer_kernel(
    ep_count, tp_count, slots,
    second, first, meta, gate_hbm, up_hbm, down_hbm, sgate, sup, sdown,
    out, gath1,
    gath2, metag, sbuf, disp, back, sides, psend, gate, up, down, hidden, hexp,
    own_sem, w_sem, s2, r2, sm, rm, s1, r1, sd, rd, sb, rb, sp, rs,
):
    grp, ep, tp = lax.axis_index("grp"), lax.axis_index("ep"), lax.axis_index("tp")
    rows, width = second.shape
    experts = meta.shape[0] // 2
    total = ep_count * slots
    entry_barrier(grp, ep, tp, ep_count, tp_count)
    own_copies = [
        pltpu.make_async_copy(second, gath2.at[tp], own_sem.at[0]),
        pltpu.make_async_copy(meta, metag.at[tp], own_sem.at[1]),
        pltpu.make_async_copy(first, gath1.at[tp], own_sem.at[2]),
    ]
    weight_copies = [
        pltpu.make_async_copy(gate_hbm.at[0], gate, w_sem.at[0]),
        pltpu.make_async_copy(up_hbm.at[0], up, w_sem.at[1]),
        pltpu.make_async_copy(down_hbm.at[0], down, w_sem.at[2]),
    ]

    def toward(side):
        return (grp, ep, tp + (1 if side == 0 else -1))

    def exists(side):
        return tp < tp_count - 1 if side == 0 else tp > 0

    def peer(d):
        return (grp, lax.rem(ep + d, ep_count), tp)

    def spans(body, size=CHUNK, extent=width):
        def step(c, carry):
            body(pl.ds(pl.multiple_of(c * size, size), size))
            return carry

        lax.fori_loop(0, extent // size, step, 0)

    def send_second(side, block, own):
        return [
            remote(second if own else gath2.at[block], gath2.at[block], s2.at[side, block], r2.at[block], toward(side)),
            remote(meta if own else metag.at[block], metag.at[block], sm.at[side, block], rm.at[block], toward(side)),
        ]

    def send_first(side, block, own):
        return remote(first if own else gath1.at[block], gath1.at[block], s1.at[side, block], r1.at[block], toward(side))

    def start_own_first(side, step):
        last = tp if side == 0 else tp_count - 1 - tp

        @pl.when(exists(side) & (step == last))
        def _():
            send_first(side, tp, True).start()

    def dispatch_copy(block, d):
        part = pl.ds(d * slots, slots)
        return remote(sbuf.at[block, part], disp.at[block, part], sd.at[block, d], rd.at[block, d], peer(d))

    def return_copy(block, d):
        part = pl.ds(d * slots, slots)
        return remote(sbuf.at[block, part], back.at[block, part], sb.at[block, d], rb.at[block, d], peer(ep_count - d))

    parts = width // CHUNK

    def part_span(part):
        return pl.ds(pl.multiple_of(part * CHUNK, CHUNK), CHUNK)

    def pass_on(side, block, part):
        span = part_span(part)
        return remote(
            psend.at[block, :, span], sides.at[side, block, :, span],
            sp.at[block, part], rs.at[side, block, part], toward(side),
        )

    def places_of(block, d):
        expert = lax.rem(ep + d, ep_count) * tp_count + tp
        slot_ids = lax.broadcasted_iota(jnp.int32, (slots, rows), 0).astype(jnp.float32)
        return slot_ids == metag[block, pl.ds(expert, 1), :], expert

    def process(block):
        picks = [jnp.where(places_of(block, d)[0], 1.0, 0.0) for d in range(ep_count)]
        pick = jnp.concatenate(picks, axis=0).astype(jnp.bfloat16)

        def columns(span):
            picked = jnp.dot(pick, gath2[block, :, span], preferred_element_type=jnp.float32).astype(jnp.bfloat16)
            disp[block, 0:slots, span] = picked[0:slots]
            sbuf[block, slots:total, span] = picked[slots:total]

        spans(columns)
        for d in range(1, ep_count):
            dispatch_copy(block, d).start()

    def shared_hidden(block):
        values = gath2[block]
        gated = jnp.dot(values, sgate[...], preferred_element_type=jnp.float32)
        lifted = jnp.dot(values, sup[...], preferred_element_type=jnp.float32)
        hidden[block] = (jax.nn.silu(gated) * lifted).astype(jnp.bfloat16)

    def expert(block):
        for d in range(1, ep_count):
            dispatch_copy(block, d).wait()

        def units(span):
            values = disp[block]
            gated = jnp.dot(values, gate[:, span], preferred_element_type=jnp.float32)
            lifted = jnp.dot(values, up[:, span], preferred_element_type=jnp.float32)
            hexp[:, span] = (jax.nn.silu(gated) * lifted).astype(jnp.bfloat16)

        spans(units, 256, gate.shape[1])

        def columns(span):
            result = jnp.dot(hexp[...], down[:, span], preferred_element_type=jnp.float32).astype(jnp.bfloat16)
            back[block, 0:slots, span] = result[0:slots]
            sbuf[block, slots:total, span] = result[slots:total]

        spans(columns)

    def give_back(block):
        for d in range(1, ep_count):
            return_copy(block, d).start()

    def experts_at(distance):
        def one(side, carry):
            block = tp + (2 * side - 1) * distance

            @pl.when((block >= 0) & (block < tp_count) & ((distance > 0) | (side == 0)))
            def _():
                expert(block)

                @pl.when(block != tp)
                def _():
                    give_back(block)

            return carry

        lax.fori_loop(0, 2, one, 0)

    for side in range(2):

        @pl.when(exists(side))
        def _():
            for copy in send_second(side, tp, True):
                copy.start()

        start_own_first(side, 0)
    for copy in own_copies + weight_copies:
        copy.start()

    @pl.when(tp == 0)
    def _():
        sides[0] = jnp.zeros(sides.shape[1:], sides.dtype)

    @pl.when(tp == tp_count - 1)
    def _():
        sides[1] = jnp.zeros(sides.shape[1:], sides.dtype)

    own_copies[0].wait()
    own_copies[1].wait()
    process(tp)
    shared_hidden(tp)
    for copy in weight_copies:
        copy.wait()

    def hop(k, carry):
        for side in range(2):
            block = tp - k if side == 0 else tp + k
            inside = block >= 0 if side == 0 else block < tp_count

            @pl.when(inside)
            def _():
                for copy in send_second(side, block, False):
                    copy.wait_recv()

                @pl.when(exists(side))
                def _():
                    for copy in send_second(side, block, False):
                        copy.start()

            start_own_first(side, k)

            @pl.when(inside)
            def _():
                process(block)
                shared_hidden(block)

        experts_at(k - 1)
        return carry

    lax.fori_loop(1, tp_count, hop, 0)
    own_copies[2].wait()

    def partial_of(block):
        pieces = []
        for d in range(ep_count):
            hit, number = places_of(block, d)
            pieces.append(jnp.where(hit, metag[block, pl.ds(experts + number, 1), :], 0.0))
        weights = jnp.concatenate(pieces, axis=0)
        high = weights.astype(jnp.bfloat16)
        low = (weights - high.astype(jnp.float32)).astype(jnp.bfloat16)
        turned = (((0,), (0,)), ((), ()))

        def value(span):
            picked = back[block, :, span]
            return (
                lax.dot_general(high, picked, turned, preferred_element_type=jnp.float32)
                + lax.dot_general(low, picked, turned, preferred_element_type=jnp.float32)
                + jnp.dot(hidden[block], sdown[:, span], preferred_element_type=jnp.float32)
            )

        return value

    def wait_return(block):
        for d in range(1, ep_count):
            return_copy(block, d).wait_recv()

    def reduce_step(step):
        for side in range(2):
            block = step - tp if side == 0 else 2 * (tp_count - 1) - step - tp
            active = (block > tp) & (block < tp_count) if side == 0 else (block < tp) & (block >= 0)

            @pl.when(active)
            def _():
                wait_return(block)
                value = partial_of(block)

                def one_part(part, carry):
                    span = part_span(part)
                    own = value(span)

                    @pl.when(tp > 0 if side == 0 else tp < tp_count - 1)
                    def _():
                        pass_on(side, block, part).wait_recv()

                    psend[block, :, span] = (
                        own + sides[side, block, :, span].astype(jnp.float32)
                    ).astype(jnp.bfloat16)
                    pass_on(side, block, part).start()
                    return carry

                lax.fori_loop(0, parts, one_part, 0)

    def hop_first(k, carry):
        for side in range(2):
            block = tp - k if side == 0 else tp + k
            inside = block >= 0 if side == 0 else block < tp_count

            @pl.when(inside)
            def _():
                send_first(side, block, False).wait_recv()

                @pl.when(exists(side))
                def _():
                    send_first(side, block, False).start()

        @pl.when(k == 1)
        def _():
            experts_at(tp_count - 1)
            give_back(tp)

        reduce_step(2 * k - 1)
        reduce_step(2 * k)
        return carry

    lax.fori_loop(1, tp_count, hop_first, 0)
    wait_return(tp)
    own_value = partial_of(tp)

    def last_part(part, carry):
        span = part_span(part)
        own = own_value(span)

        @pl.when(tp > 0)
        def _():
            pass_on(0, tp, part).wait_recv()

        @pl.when(tp < tp_count - 1)
        def _():
            pass_on(1, tp, part).wait_recv()

        out[:, span] = (
            own
            + sides[0, tp, :, span].astype(jnp.float32)
            + sides[1, tp, :, span].astype(jnp.float32)
        ).astype(jnp.bfloat16)
        return carry

    lax.fori_loop(0, parts, last_part, 0)

    def finish(block, carry):
        for d in range(1, ep_count):
            return_copy(block, d).wait_send()
        for side in range(2):
            passed = block <= tp if side == 0 else block >= tp
            summed = block > tp if side == 0 else block < tp

            @pl.when(exists(side) & passed)
            def _():
                for copy in send_second(side, block, False):
                    copy.wait_send()
                send_first(side, block, False).wait_send()

            @pl.when(summed)
            def _():
                for part in range(parts):
                    pass_on(side, block, part).wait_send()

        return carry

    lax.fori_loop(0, tp_count, finish, 0)


def layer(second, first, meta, gate, up, down, sgate, sup, sdown, ep_count, tp_count, slots):
    rows, width = second.shape
    vmem = pl.BlockSpec(memory_space=pltpu.VMEM)
    hbm = pl.BlockSpec(memory_space=pl.ANY)
    dma = pltpu.SemaphoreType.DMA
    bf16 = jnp.bfloat16
    total = ep_count * slots
    return pl.pallas_call(
        functools.partial(layer_kernel, ep_count, tp_count, slots),
        out_shape=(
            jax.ShapeDtypeStruct((rows, width), bf16),
            jax.ShapeDtypeStruct((tp_count, rows, width), bf16),
        ),
        in_specs=[vmem] * 3 + [hbm] * 3 + [vmem] * 3,
        out_specs=(vmem, vmem),
        scratch_shapes=[
            pltpu.VMEM((tp_count, rows, width), bf16),
            pltpu.VMEM((tp_count,) + meta.shape, jnp.float32),
            pltpu.VMEM((tp_count, total, width), bf16),
            pltpu.VMEM((tp_count, total, width), bf16),
            pltpu.VMEM((tp_count, total, width), bf16),
            pltpu.VMEM((2, tp_count, rows, width), bf16),
            pltpu.VMEM((tp_count, rows, width), bf16),
            pltpu.VMEM(gate.shape[1:], bf16),
            pltpu.VMEM(up.shape[1:], bf16),
            pltpu.VMEM(down.shape[1:], bf16),
            pltpu.VMEM((tp_count, rows, sgate.shape[1]), bf16),
            pltpu.VMEM((total, gate.shape[2]), bf16),
            dma((3,)),
            dma((3,)),
            dma((2, tp_count)),
            dma((tp_count,)),
            dma((2, tp_count)),
            dma((tp_count,)),
            dma((2, tp_count)),
            dma((tp_count,)),
            dma((tp_count, ep_count)),
            dma((tp_count, ep_count)),
            dma((tp_count, ep_count)),
            dma((tp_count, ep_count)),
            dma((tp_count, width // CHUNK)),
            dma((2, tp_count, width // CHUNK)),
        ],
        compiler_params=pltpu.CompilerParams(
            collective_id=0, has_side_effects=True, vmem_limit_bytes=VMEM_LIMIT
        ),
        name="layer",
    )(second, first, meta, gate, up, down, sgate, sup, sdown)


def body(
    mixer_in,
    mixer_gain,
    w_query,
    w_key,
    w_value,
    sink_logit,
    moe_in,
    moe_gain,
    router,
    routes,
    expert_gate,
    expert_up,
    expert_down,
    shared_gate,
    shared_up,
    shared_down,
):
    tokens = mixer_in.shape[0]
    ep_count, tp_count = lax.axis_size("ep"), lax.axis_size("tp")
    top_count = routes.shape[1]
    experts = router.shape[1]
    capacity = 3 * top_count * tokens // (2 * experts)
    slots = -(-capacity // 16) * 16
    normed_second = rms_rows(moe_in, moe_gain)
    normed_first = rms_rows(mixer_in, mixer_gain)
    affinity = jax.nn.sigmoid(jnp.dot(normed_second, router, preferred_element_type=jnp.float32))
    hits = jnp.any(
        routes[:, :, None] == jnp.arange(experts, dtype=jnp.int32)[None, None, :], axis=1
    )
    chosen = jnp.where(hits, affinity, 0.0)
    route_weight = ROUTED_SCALE * chosen / jnp.sum(chosen, axis=-1, keepdims=True)
    earlier = jnp.tril(jnp.ones((tokens, tokens), jnp.bfloat16), -1)
    before = jnp.dot(earlier, hits.astype(jnp.bfloat16), preferred_element_type=jnp.float32)
    places = jnp.where(hits, before, -1.0)
    meta = jnp.concatenate([places, route_weight], axis=1).T
    width = normed_second.shape[1]
    moe_out, gathered_first = layer(
        normed_second, normed_first, meta, expert_gate, expert_up, expert_down,
        shared_gate, shared_up, shared_down, ep_count, tp_count, slots,
    )
    query_cols = w_query.shape[1]
    key_cols = w_key.shape[1]
    joined = jnp.concatenate([w_query, w_key, w_value], axis=1)
    projected = jnp.dot(
        gathered_first.reshape(-1, width), joined, preferred_element_type=jnp.float32
    )
    span_rows = projected.shape[0]
    offset = lax.axis_index("ep") * span_rows
    seq_length = span_rows * ep_count
    positions = offset + jnp.arange(span_rows, dtype=jnp.int32)
    query_rows = rotate(
        projected[:, :query_cols].reshape(span_rows, -1, HEAD_DIM), positions
    ).astype(jnp.bfloat16)
    key_rows = rotate(
        projected[:, query_cols : query_cols + key_cols].reshape(span_rows, -1, HEAD_DIM), positions
    ).astype(jnp.bfloat16)
    value_rows = projected[:, query_cols + key_cols :].astype(jnp.bfloat16)
    stacked = jnp.concatenate([key_rows.reshape(span_rows, key_cols), value_rows], axis=1)
    padded = extended(stacked, (("ep", 0),), WINDOW)
    mixed = attend(query_rows, padded, sink_logit, offset, seq_length)
    return (mixed, moe_out)


def solution(mesh):
    return jax.shard_map(
        body,
        mesh=mesh,
        in_specs=(
            P(("grp", "ep", "tp"), None),
            P(),
            P(None, "tp"),
            P(None, "tp"),
            P(None, "tp"),
            P("tp"),
            P(("grp", "ep", "tp"), None),
            P(),
            P(),
            P(("grp", "ep", "tp"), None),
            P(("ep", "tp"), None, None),
            P(("ep", "tp"), None, None),
            P(("ep", "tp"), None, None),
            P(None, "tp"),
            P(None, "tp"),
            P("tp", None),
        ),
        out_specs=(P(("grp", "ep"), "tp"), P(("grp", "ep", "tp"), None)),
        check_vma=False,
    )
```

```python
import functools

import jax
import jax.numpy as jnp
from jax import lax
from jax.experimental import pallas as pl
from jax.experimental.pallas import tpu as pltpu
from jax.sharding import PartitionSpec as P

HEAD_DIM = 64
WINDOW = 128


EPS = 1e-06
THETA = 10000.0
ROUTED_SCALE = 2.5


def extended(block, sides, width):
    for axis, dim in sides:
        count = lax.axis_size(axis)
        forward = [(i, i + 1) for i in range(count - 1)]
        backward = [(target, source) for source, target in forward]
        low = lax.ppermute(
            lax.slice_in_dim(block, block.shape[dim] - width, None, axis=dim), axis, forward
        )
        high = lax.ppermute(lax.slice_in_dim(block, 0, width, axis=dim), axis, backward)
        block = jnp.concatenate([low, block, high], axis=dim)
    return block


def rms_rows(row_block, gain_vector):
    values = row_block.astype(jnp.float32)
    factor = lax.rsqrt(jnp.mean(values * values, axis=-1, keepdims=True) + EPS)
    return (values * factor * gain_vector).astype(jnp.bfloat16)


def rotate(head_rows, positions):
    half_width = head_rows.shape[-1] // 2
    inverse = THETA ** (-(jnp.arange(half_width, dtype=jnp.float32) * 2.0) / head_rows.shape[-1])
    angles = positions.astype(jnp.float32)[:, None] * inverse[None, :]
    cosine_table = jnp.cos(angles)[:, None, :]
    sine_table = jnp.sin(angles)[:, None, :]
    first_half = head_rows[..., :half_width]
    second_half = head_rows[..., half_width:]
    return jnp.concatenate(
        [
            first_half * cosine_table - second_half * sine_table,
            second_half * cosine_table + first_half * sine_table,
        ],
        axis=-1,
    )


def attend(query_rows, stacked, sink_logit, offset, seq_length):
    span_rows, head_count, head_width = query_rows.shape
    kv_local = stacked.shape[1] // (2 * head_width)
    group_size = head_count // kv_local
    key_table = stacked[:, : kv_local * head_width].reshape(-1, kv_local, head_width)
    value_table = stacked[:, kv_local * head_width :].reshape(-1, kv_local, head_width)
    block_rows = 512
    grouped = query_rows.reshape(span_rows, kv_local, group_size, head_width)
    row_ids = jnp.arange(block_rows, dtype=jnp.int32)[:, None]
    col_ids = jnp.arange(block_rows + 2 * WINDOW, dtype=jnp.int32)[None, :]
    sink_table = sink_logit.reshape(kv_local, group_size)[:, :, None, None]

    def one_block(block_index):
        block_start = block_index * block_rows
        query_block = lax.dynamic_slice_in_dim(grouped, block_start, block_rows, 0)
        key_block = lax.dynamic_slice_in_dim(key_table, block_start, block_rows + 2 * WINDOW, 0)
        value_block = lax.dynamic_slice_in_dim(value_table, block_start, block_rows + 2 * WINDOW, 0)
        scores = jnp.einsum(
            "qkgd,ckd->kgqc", query_block, key_block, preferred_element_type=jnp.float32
        ) * head_width ** (-0.5)
        key_pos = offset + block_start - WINDOW + col_ids
        query_pos = offset + block_start + row_ids
        in_window = (
            (jnp.abs(key_pos - query_pos) <= WINDOW) & (key_pos >= 0) & (key_pos < seq_length)
        )
        scores = jnp.where(in_window[None, None], scores, -jnp.inf)
        row_max = jnp.maximum(jnp.max(scores, axis=-1, keepdims=True), sink_table)
        weights = jnp.exp(scores - row_max)
        denominator = jnp.sum(weights, axis=-1, keepdims=True) + jnp.exp(sink_table - row_max)
        probability = (weights / denominator).astype(jnp.bfloat16)
        output = jnp.einsum(
            "kgqc,ckd->qkgd", probability, value_block, preferred_element_type=jnp.float32
        )
        return output.reshape(block_rows, head_count * head_width).astype(jnp.bfloat16)

    blocks_out = lax.map(one_block, jnp.arange(span_rows // block_rows, dtype=jnp.int32))
    return blocks_out.reshape(span_rows, head_count * head_width)


MESH = pl.DeviceIdType.MESH
VMEM_LIMIT = 63 * 2**20
CHUNK = 512


def remote(src, dst, send_sem, recv_sem, device):
    return pltpu.make_async_remote_copy(
        src_ref=src,
        dst_ref=dst,
        send_sem=send_sem,
        recv_sem=recv_sem,
        device_id=device,
        device_id_type=MESH,
    )


def entry_barrier(grp, ep, tp, ep_count, tp_count):
    barrier = pltpu.get_barrier_semaphore()

    @pl.when(tp > 0)
    def _():
        pl.semaphore_signal(barrier, inc=1, device_id=(grp, ep, tp - 1), device_id_type=MESH)

    @pl.when(tp < tp_count - 1)
    def _():
        pl.semaphore_signal(barrier, inc=1, device_id=(grp, ep, tp + 1), device_id_type=MESH)

    for d in range(1, ep_count):
        pl.semaphore_signal(
            barrier, inc=1, device_id=(grp, lax.rem(ep + d, ep_count), tp), device_id_type=MESH
        )

    inner = (tp > 0) & (tp < tp_count - 1)
    pl.semaphore_wait(barrier, ep_count + jnp.where(inner, 1, 0))


def layer_kernel(
    ep_count, tp_count, slots,
    second, first, meta, gate_hbm, up_hbm, down_hbm, sgate, sup, sdown, wq, wk, wv,
    out, query, key, value_rows,
    gath1, gath2, metag, sbuf, disp, back, sides, psend, gate, up, down, hidden, hexp,
    own_sem, w_sem, s2, r2, sm, rm, s1, r1, sd, rd, sb, rb, sp, rs,
):
    grp, ep, tp = lax.axis_index("grp"), lax.axis_index("ep"), lax.axis_index("tp")
    rows, width = second.shape
    experts = meta.shape[0] // 2
    total = ep_count * slots
    entry_barrier(grp, ep, tp, ep_count, tp_count)
    own_copies = [
        pltpu.make_async_copy(second, gath2.at[tp], own_sem.at[0]),
        pltpu.make_async_copy(meta, metag.at[tp], own_sem.at[1]),
        pltpu.make_async_copy(first, gath1.at[tp], own_sem.at[2]),
    ]
    weight_copies = [
        pltpu.make_async_copy(gate_hbm.at[0], gate, w_sem.at[0]),
        pltpu.make_async_copy(up_hbm.at[0], up, w_sem.at[1]),
        pltpu.make_async_copy(down_hbm.at[0], down, w_sem.at[2]),
    ]

    def toward(side):
        return (grp, ep, tp + (1 if side == 0 else -1))

    def exists(side):
        return tp < tp_count - 1 if side == 0 else tp > 0

    def peer(d):
        return (grp, lax.rem(ep + d, ep_count), tp)

    def spans(body, size=CHUNK, extent=width):
        def step(c, carry):
            body(pl.ds(pl.multiple_of(c * size, size), size))
            return carry

        lax.fori_loop(0, extent // size, step, 0)

    def send_second(side, block, own):
        return [
            remote(second if own else gath2.at[block], gath2.at[block], s2.at[side, block], r2.at[block], toward(side)),
            remote(meta if own else metag.at[block], metag.at[block], sm.at[side, block], rm.at[block], toward(side)),
        ]

    def send_first(side, block, own):
        return remote(first if own else gath1.at[block], gath1.at[block], s1.at[side, block], r1.at[block], toward(side))

    def start_own_first(side, step):
        last = tp if side == 0 else tp_count - 1 - tp

        @pl.when(exists(side) & (step == last))
        def _():
            send_first(side, tp, True).start()

    def dispatch_copy(block, d):
        part = pl.ds(d * slots, slots)
        return remote(sbuf.at[block, part], disp.at[block, part], sd.at[block, d], rd.at[block, d], peer(d))

    def return_copy(block, d):
        part = pl.ds(d * slots, slots)
        return remote(sbuf.at[block, part], back.at[block, part], sb.at[block, d], rb.at[block, d], peer(ep_count - d))

    parts = width // CHUNK

    def part_span(part):
        return pl.ds(pl.multiple_of(part * CHUNK, CHUNK), CHUNK)

    def pass_on(side, block, part):
        span = part_span(part)
        return remote(
            psend.at[block, :, span], sides.at[side, block, :, span],
            sp.at[block, part], rs.at[side, block, part], toward(side),
        )

    def places_of(block, d):
        expert = lax.rem(ep + d, ep_count) * tp_count + tp
        slot_ids = lax.broadcasted_iota(jnp.int32, (slots, rows), 0).astype(jnp.float32)
        return slot_ids == metag[block, pl.ds(expert, 1), :], expert

    def process(block):
        picks = [jnp.where(places_of(block, d)[0], 1.0, 0.0) for d in range(ep_count)]
        pick = jnp.concatenate(picks, axis=0).astype(jnp.bfloat16)

        def columns(span):
            picked = jnp.dot(pick, gath2[block, :, span], preferred_element_type=jnp.float32).astype(jnp.bfloat16)
            disp[block, 0:slots, span] = picked[0:slots]
            sbuf[block, slots:total, span] = picked[slots:total]

        spans(columns)
        for d in range(1, ep_count):
            dispatch_copy(block, d).start()

    def shared_hidden(block):
        values = gath2[block]
        gated = jnp.dot(values, sgate[...], preferred_element_type=jnp.float32)
        lifted = jnp.dot(values, sup[...], preferred_element_type=jnp.float32)
        hidden[block] = (jax.nn.silu(gated) * lifted).astype(jnp.bfloat16)

    def expert(block):
        for d in range(1, ep_count):
            dispatch_copy(block, d).wait()

        def units(span):
            values = disp[block]
            gated = jnp.dot(values, gate[:, span], preferred_element_type=jnp.float32)
            lifted = jnp.dot(values, up[:, span], preferred_element_type=jnp.float32)
            hexp[:, span] = (jax.nn.silu(gated) * lifted).astype(jnp.bfloat16)

        spans(units, 256, gate.shape[1])

        def columns(span):
            result = jnp.dot(hexp[...], down[:, span], preferred_element_type=jnp.float32).astype(jnp.bfloat16)
            back[block, 0:slots, span] = result[0:slots]
            sbuf[block, slots:total, span] = result[slots:total]

        spans(columns)

    def give_back(block):
        for d in range(1, ep_count):
            return_copy(block, d).start()

    def experts_at(distance):
        def one(side, carry):
            block = tp + (2 * side - 1) * distance

            @pl.when((block >= 0) & (block < tp_count) & ((distance > 0) | (side == 0)))
            def _():
                expert(block)

                @pl.when(block != tp)
                def _():
                    give_back(block)

            return carry

        lax.fori_loop(0, 2, one, 0)

    for side in range(2):

        @pl.when(exists(side))
        def _():
            for copy in send_second(side, tp, True):
                copy.start()

        start_own_first(side, 0)
    for copy in own_copies + weight_copies:
        copy.start()

    @pl.when(tp == 0)
    def _():
        sides[0] = jnp.zeros(sides.shape[1:], sides.dtype)

    @pl.when(tp == tp_count - 1)
    def _():
        sides[1] = jnp.zeros(sides.shape[1:], sides.dtype)

    own_copies[0].wait()
    own_copies[1].wait()
    process(tp)
    shared_hidden(tp)
    for copy in weight_copies:
        copy.wait()

    def hop(k, carry):
        for side in range(2):
            block = tp - k if side == 0 else tp + k
            inside = block >= 0 if side == 0 else block < tp_count

            @pl.when(inside)
            def _():
                for copy in send_second(side, block, False):
                    copy.wait_recv()

                @pl.when(exists(side))
                def _():
                    for copy in send_second(side, block, False):
                        copy.start()

            start_own_first(side, k)

            @pl.when(inside)
            def _():
                process(block)
                shared_hidden(block)

        experts_at(k - 1)
        return carry

    lax.fori_loop(1, tp_count, hop, 0)
    own_copies[2].wait()

    def project(block):
        values = gath1[block]
        query[block] = jnp.dot(values, wq[...], preferred_element_type=jnp.float32)
        key[block] = jnp.dot(values, wk[...], preferred_element_type=jnp.float32)
        value_rows[block] = jnp.dot(
            values, wv[...], preferred_element_type=jnp.float32
        ).astype(jnp.bfloat16)

    project(tp)

    def partial_of(block):
        pieces = []
        for d in range(ep_count):
            hit, number = places_of(block, d)
            pieces.append(jnp.where(hit, metag[block, pl.ds(experts + number, 1), :], 0.0))
        weights = jnp.concatenate(pieces, axis=0)
        high = weights.astype(jnp.bfloat16)
        low = (weights - high.astype(jnp.float32)).astype(jnp.bfloat16)
        turned = (((0,), (0,)), ((), ()))

        def value(span):
            picked = back[block, :, span]
            return (
                lax.dot_general(high, picked, turned, preferred_element_type=jnp.float32)
                + lax.dot_general(low, picked, turned, preferred_element_type=jnp.float32)
                + jnp.dot(hidden[block], sdown[:, span], preferred_element_type=jnp.float32)
            )

        return value

    def wait_return(block):
        for d in range(1, ep_count):
            return_copy(block, d).wait_recv()

    def reduce_step(step):
        for side in range(2):
            block = step - tp if side == 0 else 2 * (tp_count - 1) - step - tp
            active = (block > tp) & (block < tp_count) if side == 0 else (block < tp) & (block >= 0)

            @pl.when(active)
            def _():
                wait_return(block)
                value = partial_of(block)

                def one_part(part, carry):
                    span = part_span(part)
                    own = value(span)

                    @pl.when(tp > 0 if side == 0 else tp < tp_count - 1)
                    def _():
                        pass_on(side, block, part).wait_recv()

                    psend[block, :, span] = (
                        own + sides[side, block, :, span].astype(jnp.float32)
                    ).astype(jnp.bfloat16)
                    pass_on(side, block, part).start()
                    return carry

                lax.fori_loop(0, parts, one_part, 0)

    def hop_first(k, carry):
        for side in range(2):
            block = tp - k if side == 0 else tp + k
            inside = block >= 0 if side == 0 else block < tp_count

            @pl.when(inside)
            def _():
                send_first(side, block, False).wait_recv()

                @pl.when(exists(side))
                def _():
                    send_first(side, block, False).start()

        @pl.when(k == 1)
        def _():
            experts_at(tp_count - 1)
            give_back(tp)

        reduce_step(2 * k - 1)
        reduce_step(2 * k)
        for side in range(2):
            block = tp - k if side == 0 else tp + k

            @pl.when(block >= 0 if side == 0 else block < tp_count)
            def _():
                project(block)

        return carry

    lax.fori_loop(1, tp_count, hop_first, 0)
    wait_return(tp)
    own_value = partial_of(tp)

    def last_part(part, carry):
        span = part_span(part)
        own = own_value(span)

        @pl.when(tp > 0)
        def _():
            pass_on(0, tp, part).wait_recv()

        @pl.when(tp < tp_count - 1)
        def _():
            pass_on(1, tp, part).wait_recv()

        out[:, span] = (
            own
            + sides[0, tp, :, span].astype(jnp.float32)
            + sides[1, tp, :, span].astype(jnp.float32)
        ).astype(jnp.bfloat16)
        return carry

    lax.fori_loop(0, parts, last_part, 0)

    def finish(block, carry):
        for d in range(1, ep_count):
            return_copy(block, d).wait_send()
        for side in range(2):
            passed = block <= tp if side == 0 else block >= tp
            summed = block > tp if side == 0 else block < tp

            @pl.when(exists(side) & passed)
            def _():
                for copy in send_second(side, block, False):
                    copy.wait_send()
                send_first(side, block, False).wait_send()

            @pl.when(summed)
            def _():
                for part in range(parts):
                    pass_on(side, block, part).wait_send()

        return carry

    lax.fori_loop(0, tp_count, finish, 0)


def layer(second, first, meta, gate, up, down, sgate, sup, sdown, wq, wk, wv, ep_count, tp_count, slots):
    rows, width = second.shape
    vmem = pl.BlockSpec(memory_space=pltpu.VMEM)
    hbm = pl.BlockSpec(memory_space=pl.ANY)
    dma = pltpu.SemaphoreType.DMA
    bf16 = jnp.bfloat16
    total = ep_count * slots
    return pl.pallas_call(
        functools.partial(layer_kernel, ep_count, tp_count, slots),
        out_shape=(
            jax.ShapeDtypeStruct((rows, width), bf16),
            jax.ShapeDtypeStruct((tp_count, rows, wq.shape[1]), jnp.float32),
            jax.ShapeDtypeStruct((tp_count, rows, wk.shape[1]), jnp.float32),
            jax.ShapeDtypeStruct((tp_count, rows, wv.shape[1]), bf16),
        ),
        in_specs=[vmem] * 3 + [hbm] * 3 + [vmem] * 6,
        out_specs=(vmem,) * 4,
        scratch_shapes=[
            pltpu.VMEM((tp_count, rows, width), bf16),
            pltpu.VMEM((tp_count, rows, width), bf16),
            pltpu.VMEM((tp_count,) + meta.shape, jnp.float32),
            pltpu.VMEM((tp_count, total, width), bf16),
            pltpu.VMEM((tp_count, total, width), bf16),
            pltpu.VMEM((tp_count, total, width), bf16),
            pltpu.VMEM((2, tp_count, rows, width), bf16),
            pltpu.VMEM((tp_count, rows, width), bf16),
            pltpu.VMEM(gate.shape[1:], bf16),
            pltpu.VMEM(up.shape[1:], bf16),
            pltpu.VMEM(down.shape[1:], bf16),
            pltpu.VMEM((tp_count, rows, sgate.shape[1]), bf16),
            pltpu.VMEM((total, gate.shape[2]), bf16),
            dma((3,)),
            dma((3,)),
            dma((2, tp_count)),
            dma((tp_count,)),
            dma((2, tp_count)),
            dma((tp_count,)),
            dma((2, tp_count)),
            dma((tp_count,)),
            dma((tp_count, ep_count)),
            dma((tp_count, ep_count)),
            dma((tp_count, ep_count)),
            dma((tp_count, ep_count)),
            dma((tp_count, width // CHUNK)),
            dma((2, tp_count, width // CHUNK)),
        ],
        compiler_params=pltpu.CompilerParams(
            collective_id=0, has_side_effects=True, vmem_limit_bytes=VMEM_LIMIT
        ),
        name="layer",
    )(second, first, meta, gate, up, down, sgate, sup, sdown, wq, wk, wv)


def body(
    mixer_in,
    mixer_gain,
    w_query,
    w_key,
    w_value,
    sink_logit,
    moe_in,
    moe_gain,
    router,
    routes,
    expert_gate,
    expert_up,
    expert_down,
    shared_gate,
    shared_up,
    shared_down,
):
    tokens = mixer_in.shape[0]
    ep_count, tp_count = lax.axis_size("ep"), lax.axis_size("tp")
    top_count = routes.shape[1]
    experts = router.shape[1]
    capacity = 3 * top_count * tokens // (2 * experts)
    slots = -(-capacity // 16) * 16
    normed_second = rms_rows(moe_in, moe_gain)
    normed_first = rms_rows(mixer_in, mixer_gain)
    affinity = jax.nn.sigmoid(jnp.dot(normed_second, router, preferred_element_type=jnp.float32))
    hits = jnp.any(
        routes[:, :, None] == jnp.arange(experts, dtype=jnp.int32)[None, None, :], axis=1
    )
    chosen = jnp.where(hits, affinity, 0.0)
    route_weight = ROUTED_SCALE * chosen / jnp.sum(chosen, axis=-1, keepdims=True)
    earlier = jnp.tril(jnp.ones((tokens, tokens), jnp.bfloat16), -1)
    before = jnp.dot(earlier, hits.astype(jnp.bfloat16), preferred_element_type=jnp.float32)
    places = jnp.where(hits, before, -1.0)
    meta = jnp.concatenate([places, route_weight], axis=1).T
    width = normed_second.shape[1]
    moe_out, query_part, key_part, value_part = layer(
        normed_second, normed_first, meta, expert_gate, expert_up, expert_down,
        shared_gate, shared_up, shared_down, w_query, w_key, w_value, ep_count, tp_count, slots,
    )
    key_cols = w_key.shape[1]
    span_rows = tokens * tp_count
    offset = lax.axis_index("ep") * span_rows
    seq_length = span_rows * ep_count
    positions = offset + jnp.arange(span_rows, dtype=jnp.int32)
    query_rows = rotate(
        query_part.reshape(span_rows, -1, HEAD_DIM), positions
    ).astype(jnp.bfloat16)
    key_rows = rotate(
        key_part.reshape(span_rows, -1, HEAD_DIM), positions
    ).astype(jnp.bfloat16)
    value_rows = value_part.reshape(span_rows, -1)
    stacked = jnp.concatenate([key_rows.reshape(span_rows, key_cols), value_rows], axis=1)
    padded = extended(stacked, (("ep", 0),), WINDOW)
    mixed = attend(query_rows, padded, sink_logit, offset, seq_length)
    return (mixed, moe_out)


def solution(mesh):
    return jax.shard_map(
        body,
        mesh=mesh,
        in_specs=(
            P(("grp", "ep", "tp"), None),
            P(),
            P(None, "tp"),
            P(None, "tp"),
            P(None, "tp"),
            P("tp"),
            P(("grp", "ep", "tp"), None),
            P(),
            P(),
            P(("grp", "ep", "tp"), None),
            P(("ep", "tp"), None, None),
            P(("ep", "tp"), None, None),
            P(("ep", "tp"), None, None),
            P(None, "tp"),
            P(None, "tp"),
            P("tp", None),
        ),
        out_specs=(P(("grp", "ep"), "tp"), P(("grp", "ep", "tp"), None)),
        check_vma=False,
    )
```

```python
import functools

import jax
import jax.numpy as jnp
from jax import lax
from jax.experimental import pallas as pl
from jax.experimental.pallas import tpu as pltpu
from jax.sharding import PartitionSpec as P

HEAD_DIM = 64
WINDOW = 128


EPS = 1e-06
THETA = 10000.0
ROUTED_SCALE = 2.5


def extended(block, sides, width):
    for axis, dim in sides:
        count = lax.axis_size(axis)
        forward = [(i, i + 1) for i in range(count - 1)]
        backward = [(target, source) for source, target in forward]
        low = lax.ppermute(
            lax.slice_in_dim(block, block.shape[dim] - width, None, axis=dim), axis, forward
        )
        high = lax.ppermute(lax.slice_in_dim(block, 0, width, axis=dim), axis, backward)
        block = jnp.concatenate([low, block, high], axis=dim)
    return block


def rms_rows(row_block, gain_vector):
    values = row_block.astype(jnp.float32)
    factor = lax.rsqrt(jnp.mean(values * values, axis=-1, keepdims=True) + EPS)
    return (values * factor * gain_vector).astype(jnp.bfloat16)


def rotate(flat_rows, positions):
    half_width = HEAD_DIM // 2
    channel = jnp.arange(flat_rows.shape[-1], dtype=jnp.int32) % HEAD_DIM
    place = (channel % half_width).astype(jnp.float32)
    inverse = THETA ** (-(place * 2.0) / HEAD_DIM)
    angles = positions.astype(jnp.float32)[:, None] * inverse[None, :]
    lower = (channel < half_width)[None, :]
    partner = jnp.where(
        lower, jnp.roll(flat_rows, -half_width, axis=1), jnp.roll(flat_rows, half_width, axis=1)
    )
    return flat_rows * jnp.cos(angles) + partner * jnp.where(lower, -jnp.sin(angles), jnp.sin(angles))


def attend(query_rows, stacked, sink_logit, offset, seq_length):
    span_rows, head_count, head_width = query_rows.shape
    kv_local = stacked.shape[1] // (2 * head_width)
    group_size = head_count // kv_local
    key_table = stacked[:, : kv_local * head_width].reshape(-1, kv_local, head_width)
    value_table = stacked[:, kv_local * head_width :].reshape(-1, kv_local, head_width)
    block_rows = 512
    grouped = query_rows.reshape(span_rows, kv_local, group_size, head_width)
    row_ids = jnp.arange(block_rows, dtype=jnp.int32)[:, None]
    col_ids = jnp.arange(block_rows + 2 * WINDOW, dtype=jnp.int32)[None, :]
    sink_table = sink_logit.reshape(kv_local, group_size)[:, :, None, None]

    def one_block(block_index):
        block_start = block_index * block_rows
        query_block = lax.dynamic_slice_in_dim(grouped, block_start, block_rows, 0)
        key_block = lax.dynamic_slice_in_dim(key_table, block_start, block_rows + 2 * WINDOW, 0)
        value_block = lax.dynamic_slice_in_dim(value_table, block_start, block_rows + 2 * WINDOW, 0)
        scores = jnp.einsum(
            "qkgd,ckd->kgqc", query_block, key_block, preferred_element_type=jnp.float32
        ) * head_width ** (-0.5)
        key_pos = offset + block_start - WINDOW + col_ids
        query_pos = offset + block_start + row_ids
        in_window = (
            (jnp.abs(key_pos - query_pos) <= WINDOW) & (key_pos >= 0) & (key_pos < seq_length)
        )
        scores = jnp.where(in_window[None, None], scores, -jnp.inf)
        row_max = jnp.maximum(jnp.max(scores, axis=-1, keepdims=True), sink_table)
        weights = jnp.exp(scores - row_max)
        denominator = jnp.sum(weights, axis=-1, keepdims=True) + jnp.exp(sink_table - row_max)
        probability = (weights / denominator).astype(jnp.bfloat16)
        output = jnp.einsum(
            "kgqc,ckd->qkgd", probability, value_block, preferred_element_type=jnp.float32
        )
        return output.reshape(block_rows, head_count * head_width).astype(jnp.bfloat16)

    blocks_out = lax.map(one_block, jnp.arange(span_rows // block_rows, dtype=jnp.int32))
    return blocks_out.reshape(span_rows, head_count * head_width)


MESH = pl.DeviceIdType.MESH
VMEM_LIMIT = 63 * 2**20
CHUNK = 512


def remote(src, dst, send_sem, recv_sem, device):
    return pltpu.make_async_remote_copy(
        src_ref=src,
        dst_ref=dst,
        send_sem=send_sem,
        recv_sem=recv_sem,
        device_id=device,
        device_id_type=MESH,
    )


def entry_barrier(grp, ep, tp, ep_count, tp_count):
    barrier = pltpu.get_barrier_semaphore()

    @pl.when(tp > 0)
    def _():
        pl.semaphore_signal(barrier, inc=1, device_id=(grp, ep, tp - 1), device_id_type=MESH)

    @pl.when(tp < tp_count - 1)
    def _():
        pl.semaphore_signal(barrier, inc=1, device_id=(grp, ep, tp + 1), device_id_type=MESH)

    for d in range(1, ep_count):
        pl.semaphore_signal(
            barrier, inc=1, device_id=(grp, lax.rem(ep + d, ep_count), tp), device_id_type=MESH
        )

    inner = (tp > 0) & (tp < tp_count - 1)
    pl.semaphore_wait(barrier, ep_count + jnp.where(inner, 1, 0))


def layer_kernel(
    ep_count, tp_count, slots,
    second, first, meta, gate_hbm, up_hbm, down_hbm, sgate, sup, sdown, wq, wk, wv,
    out, query, key, value_rows,
    gath1, gath2, metag, sbuf, disp, back, sides, psend, gate, up, down, hidden, hexp,
    own_sem, w_sem, s2, r2, sm, rm, s1, r1, sd, rd, sb, rb, sp, rs,
):
    grp, ep, tp = lax.axis_index("grp"), lax.axis_index("ep"), lax.axis_index("tp")
    rows, width = second.shape
    experts = meta.shape[0] // 2
    total = ep_count * slots
    entry_barrier(grp, ep, tp, ep_count, tp_count)
    own_copies = [
        pltpu.make_async_copy(second, gath2.at[tp], own_sem.at[0]),
        pltpu.make_async_copy(meta, metag.at[tp], own_sem.at[1]),
        pltpu.make_async_copy(first, gath1.at[tp], own_sem.at[2]),
    ]
    weight_copies = [
        pltpu.make_async_copy(gate_hbm.at[0], gate, w_sem.at[0]),
        pltpu.make_async_copy(up_hbm.at[0], up, w_sem.at[1]),
        pltpu.make_async_copy(down_hbm.at[0], down, w_sem.at[2]),
    ]

    def toward(side):
        return (grp, ep, tp + (1 if side == 0 else -1))

    def exists(side):
        return tp < tp_count - 1 if side == 0 else tp > 0

    def peer(d):
        return (grp, lax.rem(ep + d, ep_count), tp)

    def spans(body, size=CHUNK, extent=width):
        def step(c, carry):
            body(pl.ds(pl.multiple_of(c * size, size), size))
            return carry

        lax.fori_loop(0, extent // size, step, 0)

    def send_second(side, block, own):
        return [
            remote(second if own else gath2.at[block], gath2.at[block], s2.at[side, block], r2.at[block], toward(side)),
            remote(meta if own else metag.at[block], metag.at[block], sm.at[side, block], rm.at[block], toward(side)),
        ]

    def send_first(side, block, own):
        return remote(first if own else gath1.at[block], gath1.at[block], s1.at[side, block], r1.at[block], toward(side))

    def start_own_first(side, step):
        last = tp if side == 0 else tp_count - 1 - tp

        @pl.when(exists(side) & (step == last))
        def _():
            send_first(side, tp, True).start()

    def dispatch_copy(block, d):
        part = pl.ds(d * slots, slots)
        return remote(sbuf.at[block, part], disp.at[block, part], sd.at[block, d], rd.at[block, d], peer(d))

    def return_copy(block, d):
        part = pl.ds(d * slots, slots)
        return remote(sbuf.at[block, part], back.at[block, part], sb.at[block, d], rb.at[block, d], peer(ep_count - d))

    parts = width // CHUNK

    def part_span(part):
        return pl.ds(pl.multiple_of(part * CHUNK, CHUNK), CHUNK)

    def pass_on(side, block, part):
        span = part_span(part)
        return remote(
            psend.at[block, :, span], sides.at[side, block, :, span],
            sp.at[block, part], rs.at[side, block, part], toward(side),
        )

    def places_of(block, d):
        expert = lax.rem(ep + d, ep_count) * tp_count + tp
        slot_ids = lax.broadcasted_iota(jnp.int32, (slots, rows), 0).astype(jnp.float32)
        return slot_ids == metag[block, pl.ds(expert, 1), :], expert

    def process(block):
        picks = [jnp.where(places_of(block, d)[0], 1.0, 0.0) for d in range(ep_count)]
        pick = jnp.concatenate(picks, axis=0).astype(jnp.bfloat16)

        def columns(span):
            picked = jnp.dot(pick, gath2[block, :, span], preferred_element_type=jnp.float32).astype(jnp.bfloat16)
            disp[block, 0:slots, span] = picked[0:slots]
            sbuf[block, slots:total, span] = picked[slots:total]

        spans(columns)
        for d in range(1, ep_count):
            dispatch_copy(block, d).start()

    def shared_hidden(block):
        values = gath2[block]
        gated = jnp.dot(values, sgate[...], preferred_element_type=jnp.float32)
        lifted = jnp.dot(values, sup[...], preferred_element_type=jnp.float32)
        hidden[block] = (jax.nn.silu(gated) * lifted).astype(jnp.bfloat16)

    def expert(block):
        for d in range(1, ep_count):
            dispatch_copy(block, d).wait()

        def units(span):
            values = disp[block]
            gated = jnp.dot(values, gate[:, span], preferred_element_type=jnp.float32)
            lifted = jnp.dot(values, up[:, span], preferred_element_type=jnp.float32)
            hexp[:, span] = (jax.nn.silu(gated) * lifted).astype(jnp.bfloat16)

        spans(units, 256, gate.shape[1])

        def columns(span):
            result = jnp.dot(hexp[...], down[:, span], preferred_element_type=jnp.float32).astype(jnp.bfloat16)
            back[block, 0:slots, span] = result[0:slots]
            sbuf[block, slots:total, span] = result[slots:total]

        spans(columns)

    def give_back(block):
        for d in range(1, ep_count):
            return_copy(block, d).start()

    def experts_at(distance):
        def one(side, carry):
            block = tp + (2 * side - 1) * distance

            @pl.when((block >= 0) & (block < tp_count) & ((distance > 0) | (side == 0)))
            def _():
                expert(block)

                @pl.when(block != tp)
                def _():
                    give_back(block)

            return carry

        lax.fori_loop(0, 2, one, 0)

    for side in range(2):

        @pl.when(exists(side))
        def _():
            for copy in send_second(side, tp, True):
                copy.start()

        start_own_first(side, 0)
    for copy in own_copies + weight_copies:
        copy.start()

    @pl.when(tp == 0)
    def _():
        sides[0] = jnp.zeros(sides.shape[1:], sides.dtype)

    @pl.when(tp == tp_count - 1)
    def _():
        sides[1] = jnp.zeros(sides.shape[1:], sides.dtype)

    own_copies[0].wait()
    own_copies[1].wait()
    process(tp)
    shared_hidden(tp)
    for copy in weight_copies:
        copy.wait()

    def hop(k, carry):
        for side in range(2):
            block = tp - k if side == 0 else tp + k
            inside = block >= 0 if side == 0 else block < tp_count

            @pl.when(inside)
            def _():
                for copy in send_second(side, block, False):
                    copy.wait_recv()

                @pl.when(exists(side))
                def _():
                    for copy in send_second(side, block, False):
                        copy.start()

            start_own_first(side, k)

            @pl.when(inside)
            def _():
                process(block)
                shared_hidden(block)

        experts_at(k - 1)
        return carry

    lax.fori_loop(1, tp_count, hop, 0)
    own_copies[2].wait()

    def project(block):
        values = gath1[block]
        query[block] = jnp.dot(values, wq[...], preferred_element_type=jnp.float32)
        key[block] = jnp.dot(values, wk[...], preferred_element_type=jnp.float32)
        value_rows[block] = jnp.dot(
            values, wv[...], preferred_element_type=jnp.float32
        ).astype(jnp.bfloat16)


    def partial_of(block):
        pieces = []
        for d in range(ep_count):
            hit, number = places_of(block, d)
            pieces.append(jnp.where(hit, metag[block, pl.ds(experts + number, 1), :], 0.0))
        weights = jnp.concatenate(pieces, axis=0)
        high = weights.astype(jnp.bfloat16)
        low = (weights - high.astype(jnp.float32)).astype(jnp.bfloat16)
        turned = (((0,), (0,)), ((), ()))

        def value(span):
            picked = back[block, :, span]
            return (
                lax.dot_general(high, picked, turned, preferred_element_type=jnp.float32)
                + lax.dot_general(low, picked, turned, preferred_element_type=jnp.float32)
                + jnp.dot(hidden[block], sdown[:, span], preferred_element_type=jnp.float32)
            )

        return value

    def wait_return(block):
        for d in range(1, ep_count):
            return_copy(block, d).wait_recv()

    def reduce_step(step):
        for side in range(2):
            block = step - tp if side == 0 else 2 * (tp_count - 1) - step - tp
            active = (block > tp) & (block < tp_count) if side == 0 else (block < tp) & (block >= 0)

            @pl.when(active)
            def _():
                wait_return(block)
                value = partial_of(block)

                def one_part(part, carry):
                    span = part_span(part)
                    own = value(span)

                    @pl.when(tp > 0 if side == 0 else tp < tp_count - 1)
                    def _():
                        pass_on(side, block, part).wait_recv()

                    psend[block, :, span] = (
                        own + sides[side, block, :, span].astype(jnp.float32)
                    ).astype(jnp.bfloat16)
                    pass_on(side, block, part).start()
                    return carry

                lax.fori_loop(0, parts, one_part, 0)

    def hop_first(k, carry):
        for side in range(2):
            block = tp - k if side == 0 else tp + k
            inside = block >= 0 if side == 0 else block < tp_count

            @pl.when(inside)
            def _():
                send_first(side, block, False).wait_recv()

                @pl.when(exists(side))
                def _():
                    send_first(side, block, False).start()

        @pl.when(k == 1)
        def _():
            experts_at(tp_count - 1)
            give_back(tp)

        reduce_step(2 * k - 1)
        reduce_step(2 * k)
        for side in range(2):
            block = tp - k if side == 0 else tp + k

            @pl.when(block >= 0 if side == 0 else block < tp_count)
            def _():
                project(block)

        return carry

    lax.fori_loop(1, tp_count, hop_first, 0)
    project(tp)
    wait_return(tp)
    own_value = partial_of(tp)

    def last_part(part, carry):
        span = part_span(part)
        own = own_value(span)

        @pl.when(tp > 0)
        def _():
            pass_on(0, tp, part).wait_recv()

        @pl.when(tp < tp_count - 1)
        def _():
            pass_on(1, tp, part).wait_recv()

        out[:, span] = (
            own
            + sides[0, tp, :, span].astype(jnp.float32)
            + sides[1, tp, :, span].astype(jnp.float32)
        ).astype(jnp.bfloat16)
        return carry

    lax.fori_loop(0, parts, last_part, 0)

    def finish(block, carry):
        for d in range(1, ep_count):
            return_copy(block, d).wait_send()
        for side in range(2):
            passed = block <= tp if side == 0 else block >= tp
            summed = block > tp if side == 0 else block < tp

            @pl.when(exists(side) & passed)
            def _():
                for copy in send_second(side, block, False):
                    copy.wait_send()
                send_first(side, block, False).wait_send()

            @pl.when(summed)
            def _():
                for part in range(parts):
                    pass_on(side, block, part).wait_send()

        return carry

    lax.fori_loop(0, tp_count, finish, 0)


def layer(second, first, meta, gate, up, down, sgate, sup, sdown, wq, wk, wv, ep_count, tp_count, slots):
    rows, width = second.shape
    vmem = pl.BlockSpec(memory_space=pltpu.VMEM)
    hbm = pl.BlockSpec(memory_space=pl.ANY)
    dma = pltpu.SemaphoreType.DMA
    bf16 = jnp.bfloat16
    total = ep_count * slots
    return pl.pallas_call(
        functools.partial(layer_kernel, ep_count, tp_count, slots),
        out_shape=(
            jax.ShapeDtypeStruct((rows, width), bf16),
            jax.ShapeDtypeStruct((tp_count, rows, wq.shape[1]), jnp.float32),
            jax.ShapeDtypeStruct((tp_count, rows, wk.shape[1]), jnp.float32),
            jax.ShapeDtypeStruct((tp_count, rows, wv.shape[1]), bf16),
        ),
        in_specs=[vmem] * 3 + [hbm] * 3 + [vmem] * 6,
        out_specs=(vmem,) * 4,
        scratch_shapes=[
            pltpu.VMEM((tp_count, rows, width), bf16),
            pltpu.VMEM((tp_count, rows, width), bf16),
            pltpu.VMEM((tp_count,) + meta.shape, jnp.float32),
            pltpu.VMEM((tp_count, total, width), bf16),
            pltpu.VMEM((tp_count, total, width), bf16),
            pltpu.VMEM((tp_count, total, width), bf16),
            pltpu.VMEM((2, tp_count, rows, width), bf16),
            pltpu.VMEM((tp_count, rows, width), bf16),
            pltpu.VMEM(gate.shape[1:], bf16),
            pltpu.VMEM(up.shape[1:], bf16),
            pltpu.VMEM(down.shape[1:], bf16),
            pltpu.VMEM((tp_count, rows, sgate.shape[1]), bf16),
            pltpu.VMEM((total, gate.shape[2]), bf16),
            dma((3,)),
            dma((3,)),
            dma((2, tp_count)),
            dma((tp_count,)),
            dma((2, tp_count)),
            dma((tp_count,)),
            dma((2, tp_count)),
            dma((tp_count,)),
            dma((tp_count, ep_count)),
            dma((tp_count, ep_count)),
            dma((tp_count, ep_count)),
            dma((tp_count, ep_count)),
            dma((tp_count, width // CHUNK)),
            dma((2, tp_count, width // CHUNK)),
        ],
        compiler_params=pltpu.CompilerParams(
            collective_id=0, has_side_effects=True, vmem_limit_bytes=VMEM_LIMIT
        ),
        name="layer",
    )(second, first, meta, gate, up, down, sgate, sup, sdown, wq, wk, wv)


def body(
    mixer_in,
    mixer_gain,
    w_query,
    w_key,
    w_value,
    sink_logit,
    moe_in,
    moe_gain,
    router,
    routes,
    expert_gate,
    expert_up,
    expert_down,
    shared_gate,
    shared_up,
    shared_down,
):
    tokens = mixer_in.shape[0]
    ep_count, tp_count = lax.axis_size("ep"), lax.axis_size("tp")
    top_count = routes.shape[1]
    experts = router.shape[1]
    capacity = 3 * top_count * tokens // (2 * experts)
    slots = -(-capacity // 16) * 16
    normed_second = rms_rows(moe_in, moe_gain)
    normed_first = rms_rows(mixer_in, mixer_gain)
    affinity = jax.nn.sigmoid(jnp.dot(normed_second, router, preferred_element_type=jnp.float32))
    hits = jnp.any(
        routes[:, :, None] == jnp.arange(experts, dtype=jnp.int32)[None, None, :], axis=1
    )
    chosen = jnp.where(hits, affinity, 0.0)
    route_weight = ROUTED_SCALE * chosen / jnp.sum(chosen, axis=-1, keepdims=True)
    earlier = jnp.tril(jnp.ones((tokens, tokens), jnp.bfloat16), -1)
    before = jnp.dot(earlier, hits.astype(jnp.bfloat16), preferred_element_type=jnp.float32)
    places = jnp.where(hits, before, -1.0)
    meta = jnp.concatenate([places, route_weight], axis=1).T
    width = normed_second.shape[1]
    moe_out, query_part, key_part, value_part = layer(
        normed_second, normed_first, meta, expert_gate, expert_up, expert_down,
        shared_gate, shared_up, shared_down, w_query, w_key, w_value, ep_count, tp_count, slots,
    )
    span_rows = tokens * tp_count
    offset = lax.axis_index("ep") * span_rows
    seq_length = span_rows * ep_count
    positions = offset + jnp.arange(span_rows, dtype=jnp.int32)
    query_rows = rotate(query_part.reshape(span_rows, -1), positions).astype(jnp.bfloat16)
    query_rows = query_rows.reshape(span_rows, -1, HEAD_DIM)
    key_rows = rotate(key_part.reshape(span_rows, -1), positions).astype(jnp.bfloat16)
    value_rows = value_part.reshape(span_rows, -1)
    stacked = jnp.concatenate([key_rows, value_rows], axis=1)
    padded = extended(stacked, (("ep", 0),), WINDOW)
    mixed = attend(query_rows, padded, sink_logit, offset, seq_length)
    return (mixed, moe_out)


def solution(mesh):
    return jax.shard_map(
        body,
        mesh=mesh,
        in_specs=(
            P(("grp", "ep", "tp"), None),
            P(),
            P(None, "tp"),
            P(None, "tp"),
            P(None, "tp"),
            P("tp"),
            P(("grp", "ep", "tp"), None),
            P(),
            P(),
            P(("grp", "ep", "tp"), None),
            P(("ep", "tp"), None, None),
            P(("ep", "tp"), None, None),
            P(("ep", "tp"), None, None),
            P(None, "tp"),
            P(None, "tp"),
            P("tp", None),
        ),
        out_specs=(P(("grp", "ep"), "tp"), P(("grp", "ep", "tp"), None)),
        check_vma=False,
    )
```
